256 devices in a mesh: sp: 64 (over z, y, core), tp: 4 (over x).
Axes of the slice: x: 4, y: 4, z: 8, core: 2. Of those that a mesh axis runs over, the one named last changes fastest.
Arguments:
- stream: bfloat16 [8192, 2048], P('sp'), may hold values from -12 to 12
- out_grad: bfloat16 [8192, 2048], P('sp'), may hold values from -16 to 16
- routes: int32 [8192, 2], P('sp'), may hold values from 0 to 63, all different within a row; in each aligned block of 128 rows (0 to 127, 128 to 255, ...) at most 8 rows name the same one
- route_weight: float32 [8192, 2], P('sp'), may hold values from 0.2 to 1
- queries: bfloat16 [8192, 8, 128], P('sp', 'tp'), may hold values from -6 to 6
- key_vectors: bfloat16 [8192, 8, 128], P('sp', 'tp'), may hold values from -6 to 6
- value_vectors: bfloat16 [8192, 8, 256], P('sp', 'tp'), may hold values from -6 to 6
- log_decay: float32 [8192, 8], P('sp', 'tp'), may hold values from -1 to 0
- out_proj: bfloat16 [2048, 2048], P(None, 'tp'), may hold values from -0.125 to 0.125
- gate_weight: bfloat16 [64, 2048, 1024], P('sp', None, 'tp'), may hold values from -0.125 to 0.125
- up_weight: bfloat16 [64, 2048, 1024], P('sp', None, 'tp'), may hold values from -0.125 to 0.125
- down_weight: bfloat16 [64, 1024, 2048], P('sp', 'tp'), may hold values from -0.1875 to 0.1875
Outputs:
- gate_grad: bfloat16 [64, 2048, 1024], P('sp', None, 'tp')
- up_grad: bfloat16 [64, 2048, 1024], P('sp', None, 'tp')
- down_grad: bfloat16 [64, 1024, 2048], P('sp', 'tp')
- proj_grad: float32 [2048, 2048], P('sp', 'tp')
- query_grad: bfloat16 [8192, 8, 128], P('sp', 'tp')
- key_grad: bfloat16 [8192, 8, 128], P('sp', 'tp')
- value_grad: bfloat16 [8192, 8, 256], P('sp', 'tp')
The draws below stay inside these ranges and needn't reach their ends.
Inputs may be any that keep to these rules, and one draw needn't show every extreme that they name: `routes`: each row names two different experts. In each aligned block of 128 rows no expert is named by more than 8 rows, and in some block an expert is named by exactly 8.
All inputs are finite; a program needn't handle non-finite values.
Results may differ from the reference program's by a relative error of at most 0.025.
Values may be sent and summed in bfloat16 or wider, within the bound.
No kernel may reach another device: no remote copies, remote signals or barrier semaphores. Data moves between devices by JAX's collectives and lax.ppermute only.
A program may use at most 128 MiB of HBM per device.

```python
import math
import jax
import jax.numpy as jnp
import numpy as np
from jax import lax

D = 2048
RETENTION_HEADS = 8
KD = 128
VD = 256
FF = 1024
TOK_DEV = 128
SEQUENCE_TOKENS = 8192
EXPERTS = 64
CAP = 8
HV = 2048
N_SP = 64
N_TP = 4


def draw_log_decay(key, part):
    random_subkeys = jax.random.split(jax.random.fold_in(key, 7), 7)
    ranking = jax.random.permutation(random_subkeys[0], RETENTION_HEADS)
    slow_rate = jax.random.uniform(random_subkeys[1], (RETENTION_HEADS,), jnp.float32, 0.05, 0.2) / SEQUENCE_TOKENS
    fast_rate = jnp.exp(jax.random.uniform(random_subkeys[2], (RETENTION_HEADS,), jnp.float32, math.log(0.012), math.log(0.025)))
    baseline_decay_rate = jnp.where(ranking < RETENTION_HEADS // 2, fast_rate, slow_rate)
    decay_factor = jnp.exp(jax.random.uniform(random_subkeys[3], (SEQUENCE_TOKENS // TOK_DEV, RETENTION_HEADS), jnp.float32, 0.0, math.log(3.0)))
    decay_factor = jnp.repeat(decay_factor, TOK_DEV, axis=0)
    jitter_amount = jax.random.uniform(random_subkeys[4], (SEQUENCE_TOKENS, RETENTION_HEADS), jnp.float32, 0.6, 1.4)
    spike_location = jax.random.randint(random_subkeys[5], (2, RETENTION_HEADS), 0, SEQUENCE_TOKENS)
    spike_depth = jax.random.uniform(random_subkeys[6], (2, RETENTION_HEADS), jnp.float32, math.log(0.5), math.log(0.8))
    token_position = jnp.arange(SEQUENCE_TOKENS, dtype=jnp.int32)[:, None]
    spike_events = jnp.where(token_position == spike_location[0][None, :], spike_depth[0][None, :], 0.0)
    spike_events = spike_events + jnp.where(token_position == spike_location[1][None, :], spike_depth[1][None, :], 0.0)
    return -(baseline_decay_rate[None, :] * decay_factor * jitter_amount) + spike_events


def strengthened(drawn, own_key, source, target, shards_of, factor):
    def block_of(position):
        return (jnp.arange(drawn.shape[position]) // (drawn.shape[position] // shards_of)).reshape((-1,) + (1,) * (drawn.ndim - 1 - position))

    first = jax.random.permutation(own_key, shards_of)[block_of(target)]
    far = (block_of(target) + shards_of // 2) % shards_of
    return jnp.where((block_of(source) == first) | (block_of(source) == far), factor * drawn, drawn)


def block_levels(rng, extent, cuts, least, largest):
    loudness, own = 1.0, jax.random.fold_in(rng, 6)
    for position, blocks in cuts:
        draws = jnp.exp(jax.random.uniform(jax.random.fold_in(own, position), (blocks,), jnp.float32, least / len(cuts), largest / len(cuts)))
        loudness = loudness * jnp.repeat(draws, extent[position] // blocks).reshape([-1 if axis == position else 1 for axis in range(len(extent))])
    return loudness


def deal_out(own_key, own, number, rows, count, top, reach, skew):
    sequence = jax.random.permutation(own_key, count)
    heavy_load, common = portions_of(count, rows * top, reach, skew, True), portions_of(count, rows * top, reach, skew, False)
    places = jnp.arange(count)

    def named(sizes, rotation):
        used = int((sizes > 0).sum())
        fixed = max(1, used // 4)
        moved = fixed + (places - fixed + rotation * (used - fixed)) % max(1, count - fixed)
        return jnp.zeros((count,), jnp.int32).at[sequence[jnp.where(places < fixed, places, moved)]].set(jnp.asarray(sizes, jnp.int32))

    sizes = jnp.where(number % 4 == 0, named(heavy_load, number // 4), named(common, number - number // 4 - 1))
    mixed = jax.random.permutation(jax.random.fold_in(own, 3), count)
    donor, taker = mixed[0:count // 2 * 2:2], mixed[1:count // 2 * 2:2]
    slack = jnp.minimum(sizes[donor] - 1, reach - sizes[taker]) // 2
    slack = jnp.where((donor == sequence[0]) | (taker == sequence[0]) | (sizes[taker] == 0), 0, jnp.maximum(slack, 0))
    moved = jax.random.randint(jax.random.fold_in(own, 4), (count // 2,), 0, 1 << 20) % (slack + 1)
    sizes = sizes.at[donor].add(-moved).at[taker].add(moved)
    members = jnp.searchsorted(jnp.cumsum(sizes), jnp.arange(rows * top), side="right").astype(jnp.int32)
    listing = members.reshape(top, rows).T
    listing = listing[jax.random.permutation(jax.random.fold_in(own, 1), rows)]
    rotation = jax.random.randint(jax.random.fold_in(own, 2), (rows, 1), 0, top)
    return jnp.take_along_axis(listing, (jnp.arange(top)[None, :] + rotation) % top, axis=1)


def portions_of(number_of, total, most, skew, full):
    loads = [(1 << 20) // math.isqrt(standing ** skew) + 1 for standing in range(1, number_of + 1)]
    largest = most if full else min(most, max(-(-total // number_of), total * loads[0] // sum(loads)))
    least = 1 if total - largest >= number_of - 1 else 0
    given, spare = [largest] + [least] * (number_of - 1), total - largest - least * (number_of - 1)
    while spare > 0:
        movable = [i for i in range(1, number_of) if given[i] < largest] or [i for i in range(1, number_of) if given[i] < most]
        pool, remaining = sum([loads[i] for i in movable]), spare
        for i in movable:
            more = min(most - given[i], max(1, remaining * loads[i] // pool), spare)
            given[i] = given[i] + more
            spare = spare - more
    return np.array(given)


def bell_draw(own_key, extent, scale, limit, cuts=(), kind=jnp.bfloat16):
    level = block_levels(own_key, extent, cuts, -0.22, 0.18) if cuts else 1.0
    values = jax.random.normal(own_key, extent, jnp.float32) * scale * level
    return jnp.minimum(jnp.maximum(values, -limit), limit).astype(kind)


def gaussian_with(stream_key, shape, width, limit, cuts, heavy, kind=jnp.bfloat16):
    result = width * jax.random.normal(stream_key, shape, jnp.float32)
    if cuts:
        result = result * block_levels(stream_key, shape, cuts, -0.22, 0.18)
    return jnp.clip(strengthened(result, jax.random.fold_in(stream_key, 3), *heavy), -limit, limit).astype(kind)


def setup_inputs(seed: int = 0) -> dict:
    arg_keys = jax.random.split(jax.random.key(seed), 13)
    stream = bell_draw(arg_keys[0], (SEQUENCE_TOKENS, D), 2.5, 12.0, ((0, 64),))
    out_grad = gaussian_with(arg_keys[1], (SEQUENCE_TOKENS, D), 1.0, 16.0, ((0, 64),), (0, 1, 64, 4.0))
    routes_keys = jax.random.split(jax.random.fold_in(arg_keys[2], 1), SEQUENCE_TOKENS // TOK_DEV)
    routes_turns = jax.random.permutation(jax.random.fold_in(arg_keys[2], 3), SEQUENCE_TOKENS // TOK_DEV)
    routes = jax.vmap(lambda own, number: deal_out(jax.random.fold_in(arg_keys[2], 2), own, number, TOK_DEV, EXPERTS, 2, CAP, 1))(routes_keys, routes_turns).reshape((SEQUENCE_TOKENS, 2))
    route_weight = jnp.clip(jnp.exp(math.log(1.0) - 1.609438 * jax.random.uniform(arg_keys[3], (SEQUENCE_TOKENS, 2), jnp.float32) ** block_levels(arg_keys[3], (SEQUENCE_TOKENS, 2), ((0, 64),), -0.2, 0.2)), 0.2, 1.0)
    queries = bell_draw(arg_keys[4], (SEQUENCE_TOKENS, RETENTION_HEADS, KD), 1.0, 6.0, ((0, 64), (1, 4)))
    key_vectors = bell_draw(arg_keys[5], (SEQUENCE_TOKENS, RETENTION_HEADS, KD), 1.0, 6.0, ((0, 64), (1, 4)))
    value_vectors = bell_draw(arg_keys[6], (SEQUENCE_TOKENS, RETENTION_HEADS, VD), 1.0, 6.0, ((0, 64), (1, 4)))
    log_decay = draw_log_decay(jax.random.fold_in(arg_keys[12], 71), 0)
    out_proj = bell_draw(arg_keys[8], (D, HV), HV ** -0.5, 0.125, ((1, 4),))
    gate_weight = bell_draw(arg_keys[9], (EXPERTS, D, FF), D ** -0.5, 0.125, ((0, 64), (2, 4)))
    up_weight = bell_draw(arg_keys[10], (EXPERTS, D, FF), D ** -0.5, 0.125, ((0, 64), (2, 4)))
    down_weight = bell_draw(arg_keys[11], (EXPERTS, FF, D), FF ** -0.5, 0.1875, ((0, 64), (1, 4)))
    return dict(stream=stream, out_grad=out_grad, routes=routes, route_weight=route_weight, queries=queries, key_vectors=key_vectors, value_vectors=value_vectors, log_decay=log_decay, out_proj=out_proj, gate_weight=gate_weight, up_weight=up_weight, down_weight=down_weight)


CLAMP_LIMIT = 7.0
GATE_SLOPE = 1.702
EPSILON = 1e-06
TOP_PRECISION = lax.Precision.HIGHEST

def slot_numbers(route_block, expert_count):
    flat_ids = route_block.reshape(-1)
    onehot = (flat_ids[:, None] == jnp.arange(expert_count, dtype=jnp.int32)[None, :]).astype(jnp.int32)
    before = jnp.cumsum(onehot, axis=0) - onehot
    return (flat_ids, lax.optimization_barrier(jnp.sum(before * onehot, axis=1)).astype(jnp.int32))

def rotation_tables(start, count, key_width):
    frequency = 1.0 / 10000.0 ** jnp.linspace(0.0, 1.0, key_width // 2, dtype=jnp.float32)
    token_position = (start + jnp.arange(count, dtype=jnp.int32)).astype(jnp.float32)
    angles = token_position[:, None] * frequency[None, :]
    return (jnp.cos(angles), jnp.sin(angles))

def turn(field, cosines, sines):
    paired = field.reshape(field.shape[:-1] + (field.shape[-1] // 2, 2))
    even_part = paired[..., 0]
    odd_part = paired[..., 1]
    cos_rows = cosines[:, None, :]
    sin_rows = sines[:, None, :]
    turned = jnp.stack([even_part * cos_rows - odd_part * sin_rows, odd_part * cos_rows + even_part * sin_rows], axis=-1)
    return turned.reshape(field.shape)

def expert_pass(routed_rows, routed_grads, gate_w, up_w, down_w):
    gate_pre = jnp.dot(routed_rows, gate_w, preferred_element_type=jnp.float32)
    up_pre = jnp.dot(routed_rows, up_w, preferred_element_type=jnp.float32)
    gate_clip = jnp.minimum(gate_pre, CLAMP_LIMIT)
    up_clip = jnp.clip(up_pre, -CLAMP_LIMIT, CLAMP_LIMIT)
    sigmoid_gate = jax.nn.sigmoid(GATE_SLOPE * gate_clip)
    activated = (gate_clip * sigmoid_gate * (up_clip + 1.0)).astype(jnp.bfloat16)
    down_part = lax.dot_general(activated, routed_grads, (((0,), (0,)), ((), ())), preferred_element_type=jnp.float32)
    act_grad = lax.dot_general(routed_grads, down_w, (((1,), (1,)), ((), ())), preferred_element_type=jnp.float32)
    slope = sigmoid_gate + GATE_SLOPE * gate_clip * sigmoid_gate * (1.0 - sigmoid_gate)
    gate_pre_grad = jnp.where(gate_pre < CLAMP_LIMIT, act_grad * (up_clip + 1.0) * slope, 0.0).astype(jnp.bfloat16)
    up_pre_grad = jnp.where(jnp.abs(up_pre) < CLAMP_LIMIT, act_grad * gate_clip * sigmoid_gate, 0.0).astype(jnp.bfloat16)
    gate_part = lax.dot_general(routed_rows, gate_pre_grad, (((0,), (0,)), ((), ())), preferred_element_type=jnp.float32)
    up_part = lax.dot_general(routed_rows, up_pre_grad, (((0,), (0,)), ((), ())), preferred_element_type=jnp.float32)
    row_count = routed_rows.shape[0]
    group = gate_w.shape[1] // N_TP
    gate_groups = gate_pre_grad.reshape(row_count, N_TP, group).astype(jnp.float32)
    up_groups = up_pre_grad.reshape(row_count, N_TP, group).astype(jnp.float32)
    gate_w_groups = gate_w.reshape(gate_w.shape[0], N_TP, group).astype(jnp.float32)
    up_w_groups = up_w.reshape(up_w.shape[0], N_TP, group).astype(jnp.float32)
    partial_value = jnp.einsum('rtf,dtf->trd', gate_groups, gate_w_groups) + jnp.einsum('rtf,dtf->trd', up_groups, up_w_groups)
    rounded = lax.optimization_barrier(partial_value.astype(jnp.bfloat16))
    back_rows = lax.optimization_barrier(jnp.sum(rounded.astype(jnp.float32), axis=0)).astype(jnp.bfloat16)
    return (gate_part.astype(jnp.bfloat16), up_part.astype(jnp.bfloat16), down_part.astype(jnp.bfloat16), back_rows)

def prepare(query_block, key_block, value_block, decay_block, start):
    cosines, sines = rotation_tables(start, TOK_DEV, KD)
    query_rotated = turn(query_block.astype(jnp.float32), cosines, sines).transpose(1, 0, 2)
    key_rotated = (turn(key_block.astype(jnp.float32), cosines, sines) * KD ** (-0.5)).transpose(1, 0, 2)
    value_per_head = value_block.astype(jnp.float32).transpose(1, 0, 2)
    running_total = jnp.cumsum(decay_block, axis=0).T
    block_total = running_total[:, -1]
    causal = (jnp.arange(TOK_DEV)[:, None] >= jnp.arange(TOK_DEV)[None, :])[None]
    difference = running_total[:, :, None] - running_total[:, None, :]
    decay_mask = jnp.where(causal, jnp.exp(jnp.where(causal, difference, 0.0)), 0.0)
    return (query_rotated, key_rotated, value_per_head, running_total, block_total, decay_mask, cosines, sines)

def reference(stream, out_grad, routes, route_weight, queries, key_vectors, value_vectors, log_decay, out_proj, gate_weight, up_weight, down_weight):
    pair_count = 2 * TOK_DEV
    flat_ids, slot_ids = jax.vmap(lambda block_data: slot_numbers(block_data, EXPERTS))(routes.reshape(N_SP, TOK_DEV, 2))
    destination = flat_ids * CAP + slot_ids

    def place(target):
        return jnp.full((EXPERTS * CAP,), -1, jnp.int32).at[target].set(jnp.arange(pair_count, dtype=jnp.int32))
    source = jax.vmap(place)(destination)
    block_ids = jnp.arange(N_SP, dtype=jnp.int32)[:, None]
    present = source >= 0
    global_pair = jnp.where(present, block_ids * pair_count + source, 0).astype(jnp.int32)
    per_expert = global_pair.reshape(N_SP, EXPERTS, CAP).transpose(1, 0, 2).reshape(EXPERTS, N_SP * CAP)
    occupied = present.reshape(N_SP, EXPERTS, CAP).transpose(1, 0, 2).reshape(EXPERTS, N_SP * CAP)
    pair_grad = (route_weight[:, :, None] * out_grad[:, None, :].astype(jnp.float32)).astype(jnp.bfloat16)
    pair_grad = pair_grad.reshape(2 * SEQUENCE_TOKENS, D)
    zero_value = jnp.zeros((), jnp.bfloat16)

    def one_expert(expert_index):
        pair_ids = per_expert[expert_index]
        row_mask = occupied[expert_index][:, None]
        routed_rows = jnp.where(row_mask, jnp.take(stream, pair_ids // 2, axis=0), zero_value)
        routed_grads = jnp.where(row_mask, jnp.take(pair_grad, pair_ids, axis=0), zero_value)
        return expert_pass(routed_rows, routed_grads, gate_weight[expert_index], up_weight[expert_index], down_weight[expert_index])
    gate_grad, up_grad, down_grad, back_rows = lax.map(one_expert, jnp.arange(EXPERTS, dtype=jnp.int32))
    row_index = (flat_ids * (N_SP * CAP) + block_ids * CAP + slot_ids).astype(jnp.int32)
    per_pair = jnp.take(back_rows.reshape(EXPERTS * N_SP * CAP, D), row_index.reshape(-1), axis=0)
    per_pair = per_pair.reshape(SEQUENCE_TOKENS, 2, D).astype(jnp.float32)
    resid_grad = (out_grad.astype(jnp.float32) + per_pair[:, 0] + per_pair[:, 1]).astype(jnp.bfloat16)

    def to_blocks(array):
        return array.reshape((N_SP, TOK_DEV) + array.shape[1:])
    starts = jnp.arange(N_SP, dtype=jnp.int32) * TOK_DEV
    inputs = (to_blocks(queries), to_blocks(key_vectors), to_blocks(value_vectors), to_blocks(log_decay), starts)

    def forward(running_state, block_data):
        query_rotated, key_rotated, value_per_head, running_total, block_total, decay_mask, cosines, sines = prepare(*block_data)
        weights = jnp.einsum('hik,hjk->hij', query_rotated, key_rotated, precision=TOP_PRECISION) * decay_mask
        retained_output = jnp.einsum('hij,hjv->hiv', weights, value_per_head, precision=TOP_PRECISION)
        retained_output = retained_output + jnp.exp(running_total)[..., None] * jnp.einsum('dzr,drs->dzs', query_rotated, running_state, precision=TOP_PRECISION)
        remaining_decay = jnp.exp(block_total[:, None] - running_total)
        inner_state = jnp.einsum('wfs,wfi->wsi', key_rotated * remaining_decay[..., None], value_per_head, precision=TOP_PRECISION)
        new_state = jnp.exp(block_total)[:, None, None] * running_state + inner_state
        return (new_state, (retained_output, running_state))
    _, (retained_all, incoming_state) = lax.scan(forward, jnp.zeros((RETENTION_HEADS, KD, VD), jnp.float32), inputs)
    inverse_rms = lax.rsqrt(lax.optimization_barrier(jnp.mean(retained_all * retained_all, axis=-1, keepdims=True)) + EPSILON)
    normed = retained_all * inverse_rms
    normed_bf = normed.transpose(0, 2, 1, 3).reshape(SEQUENCE_TOKENS, HV).astype(jnp.bfloat16)
    proj_grad = lax.dot_general(resid_grad, normed_bf, (((0,), (0,)), ((), ())), preferred_element_type=jnp.float32)
    normed_grad = jnp.dot(resid_grad, out_proj, preferred_element_type=jnp.float32)
    normed_grad = normed_grad.reshape(N_SP, TOK_DEV, RETENTION_HEADS, VD).transpose(0, 2, 1, 3)
    retention_gradient = inverse_rms * (normed_grad - normed * lax.optimization_barrier(jnp.mean(normed_grad * normed, axis=-1, keepdims=True)))

    def backward(next_rows, block_data):
        block_inputs, running_state, gradient_tile = block_data
        query_rotated, key_rotated, value_per_head, running_total, block_total, decay_mask, cosines, sines = prepare(*block_inputs)
        per_head_decay = jnp.exp(running_total)
        remaining_decay = jnp.exp(block_total[:, None] - running_total)
        weights = jnp.einsum('hik,hjk->hij', query_rotated, key_rotated, precision=TOP_PRECISION) * decay_mask
        score_grad = jnp.einsum('hiv,hjv->hij', gradient_tile, value_per_head, precision=TOP_PRECISION) * decay_mask
        query_portion = jnp.einsum('hij,hjk->hik', score_grad, key_rotated, precision=TOP_PRECISION)
        query_portion = query_portion + per_head_decay[..., None] * jnp.einsum('bpl,btl->bpt', gradient_tile, running_state, precision=TOP_PRECISION)
        key_portion = jnp.einsum('hij,hik->hjk', score_grad, query_rotated, precision=TOP_PRECISION)
        key_portion = key_portion + remaining_decay[..., None] * jnp.einsum('uxn,ubn->uxb', value_per_head, next_rows, precision=TOP_PRECISION)
        value_portion = jnp.einsum('hij,hiv->hjv', weights, gradient_tile, precision=TOP_PRECISION)
        value_portion = value_portion + remaining_decay[..., None] * jnp.einsum('bui,bim->bum', key_rotated, next_rows, precision=TOP_PRECISION)
        inner_gradient = jnp.einsum('gwn,gwj->gnj', query_rotated * per_head_decay[..., None], gradient_tile, precision=TOP_PRECISION)
        earlier_grad = inner_gradient + jnp.exp(block_total)[:, None, None] * next_rows
        q_out = turn(query_portion.transpose(1, 0, 2), cosines, -sines).astype(jnp.bfloat16)
        k_out = (turn(key_portion.transpose(1, 0, 2), cosines, -sines) * KD ** (-0.5)).astype(jnp.bfloat16)
        v_out = value_portion.transpose(1, 0, 2).astype(jnp.bfloat16)
        return (earlier_grad, (q_out, k_out, v_out))
    _, (query_grad, key_grad, value_grad) = lax.scan(backward, jnp.zeros((RETENTION_HEADS, KD, VD), jnp.float32), (inputs, incoming_state, retention_gradient), reverse=True)
    query_grad = query_grad.reshape(SEQUENCE_TOKENS, RETENTION_HEADS, KD)
    key_grad = key_grad.reshape(SEQUENCE_TOKENS, RETENTION_HEADS, KD)
    value_grad = value_grad.reshape(SEQUENCE_TOKENS, RETENTION_HEADS, VD)
    return (gate_grad, up_grad, down_grad, proj_grad, query_grad, key_grad, value_grad)
```

```python
import functools

import jax
import jax.numpy as jnp
import numpy as np
from jax import lax
from jax.experimental import pallas as pl
from jax.experimental.pallas import tpu as pltpu
from jax.sharding import Mesh
from jax.sharding import PartitionSpec as P

SP = ("sp_0", "sp_1", "sp_2")
YC = ("sp_1", "sp_2")
ZAX = "sp_0"
TP = "tp"

CLAMP_LIMIT = 7.0
GATE_SLOPE = 1.702
EPSILON = 1e-06
HI = lax.Precision.HIGHEST
F32 = jnp.float32
BF = jnp.bfloat16

NN = (((1,), (0,)), ((), ()))
NT = (((1,), (1,)), ((), ()))
TN = (((0,), (0,)), ((), ()))


def mm(a, b, dims=NN):
    return lax.dot_general(a, b, dims, preferred_element_type=F32)


def mmh(a, b, dims=NN):
    return lax.dot_general(a, b, dims, precision=HI, preferred_element_type=F32)


def iota(shape, dim):
    return lax.broadcasted_iota(jnp.int32, shape, dim)


def whole(shape):
    return pl.BlockSpec(shape, lambda i, q: (0,) * len(shape))


def call(name, body, q, args, outs, in_specs=None, out_specs=None, grid=1, flops=0):
    in_specs = in_specs or {}
    out_specs = out_specs or {}
    return pl.pallas_call(
        body,
        out_shape=[jax.ShapeDtypeStruct(s, d) for s, d in outs],
        grid_spec=pltpu.PrefetchScalarGridSpec(
            num_scalar_prefetch=1,
            grid=(grid,),
            in_specs=[in_specs.get(i, whole(a.shape)) for i, a in enumerate(args)],
            out_specs=[out_specs.get(i, whole(s)) for i, (s, _) in enumerate(outs)],
        ),
        cost_estimate=pl.CostEstimate(flops=flops, bytes_accessed=0, transcendentals=0) if flops else None,
        name=name,
    )(q, *args)


def dispatch_body(q, routes, rw, stream, og, rows, grads, qt):
    n = routes.shape[0]
    slots = rows.shape[0]
    r = routes[...].astype(F32)
    w = rw[...]
    ti, tj = iota((n, n), 0), iota((n, n), 1)
    eye = ti == tj
    before = ti < tj

    def row(c):
        return jnp.sum(jnp.where(eye, c, 0.0), axis=0, keepdims=True)

    def col(c):
        return jnp.sum(jnp.where(eye, c, 0.0), axis=1, keepdims=True)

    e0, e1 = r[:, 0:1], r[:, 1:2]
    e0r, e1r = row(e0), row(e1)
    w0r, w1r = row(w[:, 0:1]), row(w[:, 1:2])

    def earlier(er):
        same = (e0 == er).astype(F32) + (e1 == er).astype(F32)
        return jnp.sum(jnp.where(before, same, 0.0), axis=0, keepdims=True)

    cap = slots // 64
    d0 = e0r * cap + earlier(e0r)
    d1 = e1r * cap + earlier(e1r) + (e0r == e1r).astype(F32)
    di = iota((slots, n), 0).astype(F32)
    q0, q1 = di == d0, di == d1
    weight = jnp.sum(jnp.where(q0, w0r, 0.0) + jnp.where(q1, w1r, 0.0), axis=1, keepdims=True)
    pick = (jnp.where(q0, 1.0, 0.0) + jnp.where(q1, 1.0, 0.0)).astype(BF)
    rows[...] = mm(pick, stream[...]).astype(BF)
    grads[...] = (mm(pick, og[...]) * weight).astype(BF)
    dl = iota((n, slots), 1).astype(F32)
    qt[0:n, :] = jnp.where(dl == col(d0), 1.0, 0.0).astype(BF)
    qt[n : 2 * n, :] = jnp.where(dl == col(d1), 1.0, 0.0).astype(BF)


def combine_body(q, ret, qt, og, resid):
    n = og.shape[0]
    back = mm(qt[...], ret[...])
    resid[...] = ((og[...].astype(F32) + back[0:n]) + back[n : 2 * n]).astype(BF)


def gate_up_body(q, r0, r1, r2, r3, g0, g1, g2, g3, u0, u1, u2, u3, act, ga, ua):
    rows = (r0, r1, r2, r3)
    gate = mm(r0[...], g0[...])
    up = mm(r0[...], u0[...])
    for r, g, u in zip(rows[1:], (g1, g2, g3), (u1, u2, u3)):
        x = r[...]
        gate = gate + mm(x, g[...])
        up = up + mm(x, u[...])
    gc = jnp.minimum(gate, CLAMP_LIMIT)
    uc = jnp.clip(up, -CLAMP_LIMIT, CLAMP_LIMIT)
    sig = 1.0 / (1.0 + jnp.exp(-GATE_SLOPE * gc))
    gs = gc * sig
    act[...] = (gs * (uc + 1.0)).astype(BF)
    slope = sig + GATE_SLOPE * gs * (1.0 - sig)
    ga[...] = jnp.where(gate < CLAMP_LIMIT, (uc + 1.0) * slope, 0.0)
    ua[...] = jnp.where(jnp.abs(up) < CLAMP_LIMIT, gs, 0.0)


def expert_back_body(
    q, x0, x1, x2, x3, d0, d1, d2, d3, g0, g1, g2, g3, u0, u1, u2, u3, ga, ua, gp, up, b0, b1, b2, b3
):
    act_grad = mm(x0[...], d0[...], NT)
    for x, d in zip((x1, x2, x3), (d1, d2, d3)):
        act_grad = act_grad + mm(x[...], d[...], NT)
    gpg = (act_grad * ga[...]).astype(BF)
    upg = (act_grad * ua[...]).astype(BF)
    gp[...] = gpg
    up[...] = upg
    for b, g, u in zip((b0, b1, b2, b3), (g0, g1, g2, g3), (u0, u1, u2, u3)):
        b[...] = (mm(gpg, g[...], NT) + mm(upg, u[...], NT)).astype(BF)


def weight_grads_body(q, r0, r1, r2, r3, x0, x1, x2, x3, gp, up, act, gw, uw, dw):
    step = pl.program_id(0)
    for k, (r, x) in enumerate(zip((r0, r1, r2, r3), (x0, x1, x2, x3))):

        @pl.when(step == k)
        def _(r=r, x=x):
            rt = r[...]
            gw[...] = mm(rt, gp[...], TN).astype(BF)
            uw[...] = mm(rt, up[...], TN).astype(BF)
            dw[...] = mm(act[...], x[...], TN).astype(BF)


def turned(x, c, s):
    even = (iota(x.shape, 1) % 2) == 0
    n = x.shape[1]
    other = jnp.where(even, -pltpu.roll(x, n - 1, 1), pltpu.roll(x, 1, 1))
    return x * c + other * s


def prepare_body(
    q, qv, kv, vv, ld, cb, sb, cr, sr, send, qr, kr, qdt, wts, dm, dec, rem, intra, cs, sn
):
    heads, n, kd = qv.shape
    vd = vv.shape[2]
    ti, tj = iota((n, n), 0), iota((n, n), 1)
    eye, causal = ti == tj, ti >= tj
    c = cb[...] * cr[...] - sb[...] * sr[...]
    s = sb[...] * cr[...] + cb[...] * sr[...]
    cs[...] = c
    sn[...] = s
    pieces = []
    extra = []
    for h in range(heads):
        col = ld[:, h : h + 1]
        rt_r = jnp.sum(jnp.where(ti <= tj, col, 0.0), axis=0, keepdims=True)
        rt_c = jnp.sum(jnp.where(eye, rt_r, 0.0), axis=1, keepdims=True)
        total = rt_r[:, n - 1 : n]
        mask = jnp.where(causal, jnp.exp(jnp.where(causal, rt_c - rt_r, 0.0)), 0.0)
        grow = jnp.exp(rt_c)
        left = jnp.exp(total - rt_c)
        qh = turned(qv[h].astype(F32), c, s)
        kh = turned(kv[h].astype(F32), c, s) * (kd**-0.5)
        vh = vv[h].astype(F32)
        inner = mmh((kh * left).T, vh)
        for u in range(vd // 128):
            pieces.append(inner[:, u * 128 : (u + 1) * 128])
        hi = total.astype(BF).astype(F32)
        mid = (total - hi).astype(BF).astype(F32)
        low = total - hi - mid
        sub = iota((16 * vd // 128, 8, 128), 1)
        extra.append(
            jnp.where(sub == 0, hi[None], jnp.where(sub == 1, mid[None], jnp.where(sub == 2, low[None], 0.0)))
        )
        w = mmh(qh, kh, NT) * mask
        intra[:, h * vd : (h + 1) * vd] = mmh(w, vh)
        qr[h] = qh
        kr[h] = kh
        qdt[h] = (qh * grow).T
        wts[h] = w
        dm[h] = mask
        dec[h] = jnp.broadcast_to(grow, (n, 128))
        rem[h] = jnp.broadcast_to(left, (n, 128))
    state = jnp.concatenate(pieces, axis=0).reshape(-1, 8, 128)
    send[...] = jnp.concatenate([state, jnp.concatenate(extra, axis=0)], axis=1).astype(BF)


def split3(x):
    hi = x.astype(BF)
    mid = (x - hi.astype(F32)).astype(BF)
    return hi, mid


def prefix_body(q, x, out, whi, wmid):
    n = x.shape[0]
    xf = x[...].astype(F32)
    logs = (xf[:, 8, :] + xf[:, 9, :] + xf[:, 10, :])[:, 0:1]
    ti, tj = iota((n, n), 0), iota((n, n), 1)
    after = jnp.where(ti > tj, logs, 0.0)
    earlier = jnp.where(tj < ti, 1.0, 0.0)
    seg = mmh(earlier, after)
    w = jnp.where(tj < ti, jnp.exp(seg), 0.0)
    big = 8 * n
    expand = jnp.where(iota((big, n), 0) // 8 == iota((big, n), 1), 1.0, 0.0)
    same = (iota((big, big), 0) % 8) == (iota((big, big), 1) % 8)
    fwd = jnp.where(same, mmh(mmh(expand, w), expand, NT), 0.0)
    bwd = jnp.where(same, mmh(mmh(expand, w, NT), expand, NT), 0.0)
    xs = xf[:, 0:8, :].reshape(big, 128).astype(BF)
    fhi, fmid = split3(fwd)
    out[...] = (mm(fhi, xs) + mm(fmid, xs)).astype(BF)
    bhi, bmid = split3(bwd)
    whi[...] = bhi
    wmid[...] = bmid


def suffix_body(q, x, whi, wmid, out):
    xs = x[...]
    out[...] = (mm(whi[...], xs) + mm(wmid[...], xs)).astype(BF)


def joined(state, h, vd):
    per = vd // 128
    base = h * per * 128
    return jnp.concatenate([state[base + u * 128 : base + (u + 1) * 128, :] for u in range(per)], axis=1)


def normed_body(q, state, qr, dec, intra, normed, nbf, inv):
    heads = qr.shape[0]
    vd = intra.shape[1] // heads
    st = state[...].astype(F32)
    for h in range(heads):
        sl = slice(h * vd, (h + 1) * vd)
        ret = intra[:, sl] + dec[h][:, 0:1] * mmh(qr[h], joined(st, h, vd))
        iv = lax.rsqrt(jnp.mean(ret * ret, axis=1, keepdims=True) + EPSILON)
        nm = ret * iv
        normed[:, sl] = nm
        nbf[:, sl] = nm.astype(BF)
        inv[h] = jnp.broadcast_to(iv, inv.shape[1:])


def inner_grad_body(q, r0, r1, r2, r3, p0, p1, p2, p3, normed, inv, qdt, rg, send):
    heads = qdt.shape[0]
    vd = normed.shape[1] // heads
    ng = mm(r0[...], p0[...])
    for r, p in zip((r1, r2, r3), (p1, p2, p3)):
        ng = ng + mm(r[...], p[...])
    for h in range(heads):
        sl = slice(h * vd, (h + 1) * vd)
        nm, g = normed[:, sl], ng[:, sl]
        m = jnp.mean(g * nm, axis=1, keepdims=True)
        grad = inv[h][:, 0:1] * (g - nm * m)
        rg[:, sl] = grad
        inner = mmh(qdt[h], grad)
        for u in range(vd // 128):
            base = (h * (vd // 128) + u) * 128
            send[base : base + 128, :] = inner[:, u * 128 : (u + 1) * 128].astype(BF)


def transpose_body(q, r0, r1, r2, r3, out):
    for k, r in enumerate((r0, r1, r2, r3)):
        block = (q[0] + k) % 4
        t = r[...].astype(F32).T.astype(BF)
        for lo in range(2):
            at = pl.multiple_of((block * 2 + lo) * 32, 32)
            for j in range(8):
                src = lo * 256 + j * 32
                out[j, pl.ds(at, 32), :] = t[src : src + 32, :]


def local_grads_body(q, rg, vv, dm, qr, kr, wts, dec, state, cs, sn, qg, kp, vp):
    heads = qr.shape[0]
    vd = vv.shape[2]
    st = state[...].astype(F32)
    c, s = cs[...], sn[...]
    for h in range(heads):
        grad = rg[:, h * vd : (h + 1) * vd]
        score = mmh(grad, vv[h].astype(F32), NT) * dm[h]
        qp = mmh(score, kr[h]) + dec[h][:, 0:1] * mmh(grad, joined(st, h, vd), NT)
        qg[h] = turned(qp, c, -s).astype(BF)
        kp[h] = mmh(score.T, qr[h])
        vp[h] = mmh(wts[h].T, grad)


def final_body(q, state, vv, kr, rem, kp, vp, cs, sn, kg, vg):
    heads, n, kd = kr.shape
    vd = vv.shape[2]
    st = state[...].astype(F32)
    c, s = cs[...], sn[...]
    for h in range(heads):
        fut = joined(st, h, vd)
        left = rem[h][:, 0:1]
        kt = kp[h] + left * mmh(vv[h].astype(F32), fut, NT)
        kg[h] = (turned(kt, c, -s) * (kd**-0.5)).astype(BF)
        vg[h] = (vp[h] + left * mmh(kr[h], fut)).astype(BF)


def proj_body(q, rt, nb, out):
    acc = mm(rt[0], nb[0])
    for k in range(1, rt.shape[0]):
        acc = acc + mm(rt[k], nb[k])
    out[...] = acc.astype(BF)


def add_parts_body(q, x, out):
    acc = x[0].astype(F32)
    for k in range(1, x.shape[0]):
        acc = acc + x[k].astype(F32)
    out[...] = acc


def add4_body(q, a, b, c, d, out):
    out[...] = (
        (a[...].astype(F32) + b[...].astype(F32)) + (c[...].astype(F32) + d[...].astype(F32))
    ).astype(BF)


def a2a(x, axes):
    return lax.all_to_all(x, axes, split_axis=0, concat_axis=0, tiled=True)


def shift(x, by):
    return lax.ppermute(x, TP, [(i, (i + by) % 4) for i in range(4)])


def around(x):
    far = shift(x, 2)
    return x, shift(x, 3), far, shift(x, 1)


def around_ring(x):
    half = x.shape[0] // 2
    left, right = shift(x, 1), shift(x, 3)
    a, b = shift(left[:half], 1), shift(right[half:], 3)
    return x, right, jnp.concatenate([a, b], axis=0), left


def block_rows(k, shape):
    return pl.BlockSpec(shape, lambda i, q, k=k: (lax.rem(q[0] + k, 4), 0))


def block_cols(k, shape):
    return pl.BlockSpec(shape, lambda i, q, k=k: (0, lax.rem(q[0] + k, 4)))


def per_device(
    stream,
    out_grad,
    routes,
    route_weight,
    queries,
    key_vectors,
    value_vectors,
    log_decay,
    out_proj,
    gate_weight,
    up_weight,
    down_weight,
):
    n, width = stream.shape
    quarter = width // 4
    slots = 512
    hidden = gate_weight.shape[2]
    heads, kd = queries.shape[1:]
    vd = value_vectors.shape[2]
    q = lax.axis_index(TP).astype(jnp.int32)[None]
    gate_w, up_w, down_w = gate_weight[0], up_weight[0], down_weight[0]

    own = pl.BlockSpec((n, quarter), lambda i, q: (0, q[0]))
    rows, grads, qt = call(
        "dispatch",
        dispatch_body,
        q,
        (routes, route_weight, stream, out_grad),
        [((slots, quarter), BF), ((slots, quarter), BF), ((2 * n, slots), BF)],
        in_specs={2: own, 3: own},
    )
    rows = a2a(rows.reshape(64, 8, quarter), SP).reshape(slots, quarter)
    grads = a2a(grads.reshape(64, 8, quarter), SP).reshape(slots, quarter)
    rows4 = around(rows)
    grads4 = around(grads)

    freq = 1.0 / 10000.0 ** jnp.linspace(0.0, 1.0, kd // 2, dtype=F32)
    freq = jnp.repeat(freq, 2)[None, :]
    base = (lax.axis_index(SP) * n).astype(F32) * freq
    angles = jnp.arange(n, dtype=F32)[:, None] * freq
    qv = queries.transpose(1, 0, 2)
    kv = key_vectors.transpose(1, 0, 2)
    vv = value_vectors.transpose(1, 0, 2)
    sq = (heads, n, 128)
    send, qr, kr, qdt, wts, dm, dec, rem, intra, cs, sn = call(
        "prepare",
        prepare_body,
        q,
        (qv, kv, vv, log_decay, jnp.cos(base), jnp.sin(base), jnp.cos(angles), jnp.sin(angles)),
        [((64, 16, 128), BF)]
        + [(sq, F32)] * 7
        + [((n, heads * vd), F32), ((n, kd), F32), ((n, kd), F32)],
    )
    got = a2a(send, SP)
    state, whi, wmid = call(
        "prefix",
        prefix_body,
        q,
        (got,),
        [((slots, 128), BF), ((slots, slots), BF), ((slots, slots), BF)],
    )
    state = a2a(state.reshape(64, 8, 128), SP).reshape(slots, 128)
    normed, nbf, inv = call(
        "normed",
        normed_body,
        q,
        (state, qr, dec, intra),
        [((n, heads * vd), F32), ((n, heads * vd), BF), (sq, F32)],
    )
    nball = a2a(jnp.broadcast_to(nbf, (8, *nbf.shape)), YC)

    wrow = (quarter, hidden)
    gspec = {k: block_rows(k, wrow) for k in range(4)}
    dspec = {k: block_cols(k, (hidden, quarter)) for k in range(4)}
    act, ga, ua = call(
        "gate_up",
        gate_up_body,
        q,
        (*rows4, *[gate_w] * 4, *[up_w] * 4),
        [((slots, hidden), BF), ((slots, hidden), F32), ((slots, hidden), F32)],
        in_specs={4 + k: s for k, s in gspec.items()} | {8 + k: s for k, s in gspec.items()},
    )
    gp, up, *back = call(
        "expert_back",
        expert_back_body,
        q,
        (*grads4, *[down_w] * 4, *[gate_w] * 4, *[up_w] * 4, ga, ua),
        [((slots, hidden), BF)] * 2 + [((slots, quarter), BF)] * 4,
        in_specs={4 + k: s for k, s in dspec.items()}
        | {8 + k: s for k, s in gspec.items()}
        | {12 + k: s for k, s in gspec.items()},
    )
    far = shift(back[2], 2)
    nxt, prv = shift(back[1], 1), shift(back[3], 3)
    gate_grad, up_grad, down_grad = call(
        "weight_grads",
        weight_grads_body,
        q,
        (*rows4, *grads4, gp, up, act),
        [((width, hidden), BF), ((width, hidden), BF), ((hidden, width), BF)],
        out_specs={
            0: pl.BlockSpec(wrow, lambda i, q: (lax.rem(q[0] + i, 4), 0)),
            1: pl.BlockSpec(wrow, lambda i, q: (lax.rem(q[0] + i, 4), 0)),
            2: pl.BlockSpec((hidden, quarter), lambda i, q: (0, lax.rem(q[0] + i, 4))),
        },
        grid=4,
    )
    (share,) = call("add4", add4_body, q, (back[0], nxt, far, prv), [((slots, quarter), BF)])
    share = a2a(share.reshape(64, 8, quarter), SP).reshape(slots, quarter)
    (resid,) = call(
        "combine",
        combine_body,
        q,
        (share, qt, out_grad),
        [((n, quarter), BF)],
        in_specs={2: own},
    )
    resid4 = around(resid)

    pspec = {4 + k: block_rows(k, (quarter, out_proj.shape[1])) for k in range(4)}
    rg, inner = call(
        "inner_grad",
        inner_grad_body,
        q,
        (*resid4, *[out_proj] * 4, normed, inv, qdt),
        [((n, heads * vd), F32), ((slots, 128), BF)],
        in_specs=pspec,
    )
    inner = a2a(inner.reshape(64, 8, 128), SP).reshape(slots, 128)
    (turned_rows,) = call("transpose", transpose_body, q, resid4, [((8, 256, n), BF)])
    turned_rows = a2a(turned_rows, YC)
    (part,) = call("proj", proj_body, q, (turned_rows, nball), [((256, nbf.shape[1]), BF)])
    part = a2a(part.reshape(8, 32, nbf.shape[1]), ZAX)
    (proj_grad,) = call("add_parts", add_parts_body, q, (part,), [((32, nbf.shape[1]), F32)])
    qg, kp, vp = call(
        "local_grads",
        local_grads_body,
        q,
        (rg, vv, dm, qr, kr, wts, dec, state, cs, sn),
        [(sq, BF), (sq, F32), ((heads, n, vd), F32)],
    )
    (future,) = call("suffix", suffix_body, q, (inner, whi, wmid), [((slots, 128), BF)])
    future = a2a(future.reshape(64, 8, 128), SP).reshape(slots, 128)
    kg, vg = call(
        "final",
        final_body,
        q,
        (future, vv, kr, rem, kp, vp, cs, sn),
        [(sq, BF), ((heads, n, vd), BF)],
    )
    return (
        gate_grad[None],
        up_grad[None],
        down_grad[None],
        proj_grad,
        qg.transpose(1, 0, 2),
        kg.transpose(1, 0, 2),
        vg.transpose(1, 0, 2),
    )


def solution(mesh):
    split = Mesh(mesh.devices.reshape(8, 4, 2, mesh.shape["tp"]), (*SP, TP))
    placed = (
        P(SP, None),
        P(SP, None),
        P(SP, None),
        P(SP, None),
        P(SP, TP, None),
        P(SP, TP, None),
        P(SP, TP, None),
        P(SP, TP),
        P(None, TP),
        P(SP, None, TP),
        P(SP, None, TP),
        P(SP, TP, None),
    )
    return jax.shard_map(
        per_device,
        mesh=split,
        in_specs=placed,
        out_specs=(
            P(SP, None, TP),
            P(SP, None, TP),
            P(SP, TP, None),
            P(SP, TP),
            P(SP, TP, None),
            P(SP, TP, None),
            P(SP, TP, None),
        ),
        check_vma=False,
    )
```

```python
import functools

import jax
import jax.numpy as jnp
import numpy as np
from jax import lax
from jax.experimental import pallas as pl
from jax.experimental.pallas import tpu as pltpu
from jax.sharding import Mesh
from jax.sharding import PartitionSpec as P

SP = ("sp_0", "sp_1", "sp_2")
YC = ("sp_1", "sp_2")
ZAX = "sp_0"
TP = "tp"

CLAMP_LIMIT = 7.0
GATE_SLOPE = 1.702
EPSILON = 1e-06
HI = lax.Precision.HIGHEST
F32 = jnp.float32
BF = jnp.bfloat16

NN = (((1,), (0,)), ((), ()))
NT = (((1,), (1,)), ((), ()))
TN = (((0,), (0,)), ((), ()))


def mm(a, b, dims=NN):
    return lax.dot_general(a, b, dims, preferred_element_type=F32)


def mmh(a, b, dims=NN):
    return lax.dot_general(a, b, dims, precision=HI, preferred_element_type=F32)


def iota(shape, dim):
    return lax.broadcasted_iota(jnp.int32, shape, dim)


def whole(shape):
    return pl.BlockSpec(shape, lambda i, q: (0,) * len(shape))


def call(name, body, q, args, outs, in_specs=None, out_specs=None, grid=1, after=(), mib=16):
    in_specs = dict(in_specs or {})
    out_specs = out_specs or {}
    used = len(args)
    args = (*args, *after)
    for i in range(used, len(args)):
        in_specs[i] = pl.BlockSpec(memory_space=pltpu.HBM)

    def kernel(q_ref, *refs):
        body(q_ref, *refs[:used], *refs[len(args) :])

    return pl.pallas_call(
        kernel,
        out_shape=[jax.ShapeDtypeStruct(s, d) for s, d in outs],
        grid_spec=pltpu.PrefetchScalarGridSpec(
            num_scalar_prefetch=1,
            grid=(grid,),
            in_specs=[in_specs.get(i, whole(a.shape)) for i, a in enumerate(args)],
            out_specs=[out_specs.get(i, whole(s)) for i, (s, _) in enumerate(outs)],
        ),
        compiler_params=pltpu.CompilerParams(vmem_limit_bytes=mib << 20),
        name=name,
    )(q, *args)


def slots_of(routes):
    n = routes.shape[1]
    ti, tj = iota((n, n), 0), iota((n, n), 1)
    eye = ti == tj
    before = ti < tj
    r = routes[...].astype(F32)

    def col(c):
        return jnp.sum(jnp.where(eye, c, 0.0), axis=1, keepdims=True)

    e0r, e1r = r[0:1], r[1:2]
    e0, e1 = col(e0r), col(e1r)

    def earlier(er):
        same = (e0 == er).astype(F32) + (e1 == er).astype(F32)
        return jnp.sum(jnp.where(before, same, 0.0), axis=0, keepdims=True)

    cap = 8
    d0 = e0r * cap + earlier(e0r)
    d1 = e1r * cap + earlier(e1r) + (e0r == e1r).astype(F32)
    return d0, d1, col


def dispatch_body(q, routes, rw, stream, og, send, qt):
    n = routes.shape[1]
    slots = qt.shape[1]
    d0, d1, col = slots_of(routes)
    w = rw[...]
    di = iota((slots, n), 0).astype(F32)
    q0, q1 = di == d0, di == d1
    weight = jnp.where(q0, w[0:1], 0.0) + jnp.where(q1, w[1:2], 0.0)
    weight = jnp.sum(weight, axis=1, keepdims=True)
    pick = (jnp.where(q0, 1.0, 0.0) + jnp.where(q1, 1.0, 0.0)).astype(BF)
    rows = mm(pick, stream[...]).reshape(64, 8, -1)
    grads = (mm(pick, og[...]) * weight).reshape(64, 8, -1)
    send[...] = jnp.concatenate([rows, grads], axis=1).astype(BF)
    dl = iota((n, slots), 1).astype(F32)
    qt[0:n, :] = jnp.where(dl == col(d0), 1.0, 0.0).astype(BF)
    qt[n : 2 * n, :] = jnp.where(dl == col(d1), 1.0, 0.0).astype(BF)


def combine_body(q, ret, qt, og, resid):
    n = og.shape[0]
    back = mm(qt[...], ret[...])
    resid[...] = ((og[...].astype(F32) + back[0:n]) + back[n : 2 * n]).astype(BF)


def gate_up_body(q, r0, r1, r2, r3, g0, g1, g2, g3, u0, u1, u2, u3, act, ga, ua):
    rows = (r0, r1, r2, r3)
    gate = mm(r0[...], g0[...])
    up = mm(r0[...], u0[...])
    for r, g, u in zip(rows[1:], (g1, g2, g3), (u1, u2, u3)):
        x = r[...]
        gate = gate + mm(x, g[...])
        up = up + mm(x, u[...])
    gc = jnp.minimum(gate, CLAMP_LIMIT)
    uc = jnp.clip(up, -CLAMP_LIMIT, CLAMP_LIMIT)
    sig = 1.0 / (1.0 + jnp.exp(-GATE_SLOPE * gc))
    gs = gc * sig
    act[...] = (gs * (uc + 1.0)).astype(BF)
    slope = sig + GATE_SLOPE * gs * (1.0 - sig)
    ga[...] = jnp.where(gate < CLAMP_LIMIT, (uc + 1.0) * slope, 0.0)
    ua[...] = jnp.where(jnp.abs(up) < CLAMP_LIMIT, gs, 0.0)


def expert_back_body(
    q, x0, x1, x2, x3, d0, d1, d2, d3, g0, g1, g2, g3, u0, u1, u2, u3, ga, ua,
    gp, up, far_lo, far_hi, right_lo, right_hi, left_lo, left_hi, mine,
):
    act_grad = mm(x0[...], d0[...], NT)
    for x, d in zip((x1, x2, x3), (d1, d2, d3)):
        act_grad = act_grad + mm(x[...], d[...], NT)
    gpg = (act_grad * ga[...]).astype(BF)
    upg = (act_grad * ua[...]).astype(BF)
    gp[...] = gpg
    up[...] = upg

    def back(g, u):
        return (mm(gpg, g[...], NT) + mm(upg, u[...], NT)).astype(BF)

    half = far_lo.shape[0]
    for lo, hi, part in ((far_lo, far_hi, back(g2, u2)), (right_lo, right_hi, back(g1, u1)), (left_lo, left_hi, back(g3, u3))):
        lo[...] = part[:half]
        hi[...] = part[half:]
    mine[...] = back(g0, u0)


def pass_on_body(q, right_lo, far_lo, left_hi, far_hi, right, left):
    right[...] = (right_lo[...].astype(F32) + far_lo[...].astype(F32)).astype(BF)
    left[...] = (left_hi[...].astype(F32) + far_hi[...].astype(F32)).astype(BF)


def share_body(q, mine, a_lo, a_hi, b_lo, b_hi, out):
    half = a_lo.shape[0]
    m = mine[...].astype(F32)
    out[:half, :] = (m[:half] + (a_lo[...].astype(F32) + b_lo[...].astype(F32))).astype(BF)
    out[half:, :] = (m[half:] + (a_hi[...].astype(F32) + b_hi[...].astype(F32))).astype(BF)


def weight_grads_body(q, r0, r1, r2, r3, x0, x1, x2, x3, gp, up, act, gw, uw, dw, token):
    token[...] = jnp.zeros(token.shape, F32)
    step = pl.program_id(0)
    for k, (r, x) in enumerate(zip((r0, r1, r2, r3), (x0, x1, x2, x3))):

        @pl.when(step == k)
        def _(r=r, x=x):
            rt = r[...]
            gw[...] = mm(rt, gp[...], TN).astype(BF)
            uw[...] = mm(rt, up[...], TN).astype(BF)
            dw[...] = mm(act[...], x[...], TN).astype(BF)


def turned(x, c, s):
    even = (iota(x.shape, 1) % 2) == 0
    n = x.shape[1]
    other = jnp.where(even, -pltpu.roll(x, n - 1, 1), pltpu.roll(x, 1, 1))
    return x * c + other * s


QR, KR, WTS, MASK, SCAL, COS, SIN, INTRA = 0, 256, 512, 768, 1024, 1152, 1280, 1408


def prepare_body(q, qv, kv, vv, ld, cb, sb, cr, sr, send, pack):
    heads, n, kd = qv.shape
    vd = vv.shape[2]
    ti, tj = iota((n, n), 0), iota((n, n), 1)
    eye, causal = ti == tj, ti >= tj
    c = cb[...] * cr[...] - sb[...] * sr[...]
    s = sb[...] * cr[...] + cb[...] * sr[...]
    pack[:, COS : COS + kd] = c
    pack[:, SIN : SIN + kd] = s
    pieces = []
    logs = jnp.zeros((1, 8, 128), F32)
    sub = iota((1, 8, 128), 1)
    scal = jnp.zeros((n, 128), F32)
    lane = iota((n, 128), 1)
    for h in range(heads):
        col = jnp.sum(jnp.where(eye, ld[h : h + 1, :], 0.0), axis=1, keepdims=True)
        rt_r = jnp.sum(jnp.where(ti <= tj, col, 0.0), axis=0, keepdims=True)
        rt_c = jnp.sum(jnp.where(eye, rt_r, 0.0), axis=1, keepdims=True)
        total = rt_r[:, n - 1 : n]
        mask = jnp.where(causal, jnp.exp(jnp.where(causal, rt_c - rt_r, 0.0)), 0.0)
        grow = jnp.exp(rt_c)
        left = jnp.exp(total - rt_c)
        qh = turned(qv[h].astype(F32), c, s)
        kh = turned(kv[h].astype(F32), c, s) * (kd**-0.5)
        vh = vv[h].astype(F32)
        inner = mmh((kh * left).T, vh)
        for u in range(vd // 128):
            pieces.append(inner[:, u * 128 : (u + 1) * 128])
        hi = total.astype(BF).astype(F32)
        mid = (total - hi).astype(BF).astype(F32)
        for k, part in enumerate((hi, mid, total - hi - mid)):
            logs = jnp.where(sub == 3 * h + k, part[None], logs)
        w = mmh(qh, kh, NT) * mask
        pack[:, INTRA + h * vd : INTRA + (h + 1) * vd] = mmh(w, vh)
        at = h * 128
        pack[:, QR + at : QR + at + 128] = qh
        pack[:, KR + at : KR + at + 128] = kh
        pack[:, WTS + at : WTS + at + 128] = w
        pack[:, MASK + at : MASK + at + 128] = mask
        scal = jnp.where(lane == h, grow, jnp.where(lane == 2 + h, left, scal))
    pack[:, SCAL : SCAL + 128] = scal
    state = jnp.concatenate(pieces, axis=0).reshape(-1, 8, 128)
    send[...] = jnp.concatenate([state, jnp.broadcast_to(logs, state.shape)], axis=1).astype(BF)


def prefix_body(q, x, out, table):
    n = x.shape[0]
    z, j = q[1], q[2]
    xf = x[...].astype(F32)
    logs = [xf[:, 8 + 3 * h, :] + xf[:, 9 + 3 * h, :] + xf[:, 10 + 3 * h, :] for h in range(2)]
    mine = jnp.where(z >= 4, logs[1], logs[0])[:, 0:1]
    ti, tj = iota((n, n), 0), iota((n, n), 1)
    after = jnp.where(ti > tj, mine, 0.0)
    seg = mmh(jnp.where(tj < ti, 1.0, 0.0), after)
    w = jnp.where(tj < ti, jnp.exp(seg), 0.0)
    acc = mmh(w, jnp.concatenate([xf[:, k, :] for k in range(8)], axis=1))
    for k in range(8):
        out[:, k, :] = acc[:, k * 128 : (k + 1) * 128]
    other = jnp.where(j >= 4, logs[1], logs[0])[:, 0:1]
    row = jnp.sum(jnp.where(ti == tj, other, 0.0), axis=0, keepdims=True)
    i, m = iota((16, n), 0), iota((16, n), 1)
    low = jnp.where(i == 8, 8 * z - 1, 8 * z + i)
    a = jnp.where((m > low) & (i < 9), row, 0.0)
    m2, c2 = iota((n, 128), 0), iota((n, 128), 1)
    high = jnp.where(c2 < 16, 8 * z + c2, 8 * (c2 - 16))
    b = jnp.where(m2 < high, 1.0, 0.0)
    decay = jnp.exp(mmh(a, b))
    i, c = iota((16, 128), 0), iota((16, 128), 1)
    used = ((c < 8) & ((i == 8) | (c > i))) | ((c == 8) & (i < 8)) | ((i == 7) & (c >= 16) & (c < 24) & (c - 16 > z))
    table[...] = jnp.where(used, decay, 0.0)


def joined(state, h, vd):
    per = vd // 128
    base = h * per * 128
    return jnp.concatenate([state[base + u * 128 : base + (u + 1) * 128, :] for u in range(per)], axis=1)


INV, QDT = 512, 640


def normed_body(q, state, pack, nbf, back):
    n = pack.shape[0]
    heads, vd = 2, 256
    st = state[...].astype(F32)
    lane = iota((n, 128), 1)
    invs = jnp.zeros((n, 128), F32)
    for h in range(heads):
        sl = slice(h * vd, (h + 1) * vd)
        qh = pack[:, QR + h * 128 : QR + (h + 1) * 128]
        grow = pack[:, SCAL + h : SCAL + h + 1]
        ret = pack[:, INTRA + h * vd : INTRA + (h + 1) * vd] + grow * mmh(qh, joined(st, h, vd))
        iv = lax.rsqrt(jnp.mean(ret * ret, axis=1, keepdims=True) + EPSILON)
        nm = ret * iv
        back[:, sl] = nm
        for k in range(nbf.shape[0]):
            nbf[k, :, sl] = nm.astype(BF)
        invs = jnp.where(lane == h, iv, invs)
        back[:, QDT + h * 128 : QDT + (h + 1) * 128] = (qh * grow).T
    back[:, INV : INV + 128] = invs


def inner_grad_body(q, r0, r1, r2, r3, p0, p1, p2, p3, back, rg, send):
    heads, vd = 2, 256
    ng = mm(r0[...], p0[...])
    for r, p in zip((r1, r2, r3), (p1, p2, p3)):
        ng = ng + mm(r[...], p[...])
    for h in range(heads):
        sl = slice(h * vd, (h + 1) * vd)
        nm, g = back[:, sl], ng[:, sl]
        m = jnp.mean(g * nm, axis=1, keepdims=True)
        grad = back[:, INV + h : INV + h + 1] * (g - nm * m)
        rg[:, sl] = grad
        inner = mmh(back[:, QDT + h * 128 : QDT + (h + 1) * 128], grad)
        for u in range(vd // 128):
            for e in range(2):
                part = inner[e * 64 : (e + 1) * 64, u * 128 : (u + 1) * 128]
                send[h * 4 + u * 2 + e, 0:64, :] = part.astype(BF)
    for k, r in enumerate((r0, r1, r2, r3)):
        block = lax.rem(q[0] + k, 4)
        t = r[...].astype(F32).T.astype(BF)
        for lo in range(2):
            at = pl.multiple_of(64 + (block * 2 + lo) * 32, 32)
            for j in range(8):
                src = lo * 256 + j * 32
                send[j, pl.ds(at, 32), :] = t[src : src + 32, :]


def local_grads_body(q, rg, vv, pack, state, qg, rest):
    n = pack.shape[0]
    heads, vd = 2, 256
    st = state[...].astype(F32)
    c, s = pack[:, COS : COS + 128], pack[:, SIN : SIN + 128]
    for h in range(heads):
        at = h * 128
        grad = rg[:, h * vd : (h + 1) * vd]
        score = mmh(grad, vv[h].astype(F32), NT) * pack[:, MASK + at : MASK + at + 128]
        grow = pack[:, SCAL + h : SCAL + h + 1]
        qp = mmh(score, pack[:, KR + at : KR + at + 128]) + grow * mmh(grad, joined(st, h, vd), NT)
        qg[h] = turned(qp, c, -s).astype(BF)
        rest[:, at : at + 128] = mmh(score.T, pack[:, QR + at : QR + at + 128])
        rest[:, 256 + h * vd : 256 + (h + 1) * vd] = mmh(pack[:, WTS + at : WTS + at + 128].T, grad)


def plane_body(q, x, nb, table, inside, send):
    blocks = x.shape[0]
    parts = [x[k, 0:64, :].astype(F32) for k in range(blocks)]
    for k in range(blocks):
        acc = jnp.zeros((64, 128), F32)
        for m in range(k + 1, blocks):
            acc = acc + table[k : k + 1, m : m + 1] * parts[m]
        inside[k] = acc
    total = jnp.zeros((64, 128), F32)
    for m in range(blocks):
        total = total + table[8:9, m : m + 1] * parts[m]
    total = total.astype(BF)
    proj = mm(x[0, 64:320, :], nb[0])
    for k in range(1, blocks):
        proj = proj + mm(x[k, 64:320, :], nb[k])
    for k in range(blocks):
        send[k, 0:64, :] = total
        for u in range(4):
            send[k, 64 + u * 32 : 96 + u * 32, :] = proj[k * 32 : (k + 1) * 32, u * 128 : (u + 1) * 128].astype(BF)


def planes_body(q, y, inside, table, out, proj):
    blocks = y.shape[0]
    later = jnp.zeros((64, 128), F32)
    for k in range(blocks):
        later = later + table[7:8, 16 + k : 17 + k] * y[k, 0:64, :].astype(F32)
    for k in range(blocks):
        out[k] = (inside[k] + table[k : k + 1, 8:9] * later).astype(BF)
    for u in range(4):
        acc = y[0, 64 + u * 32 : 96 + u * 32, :].astype(F32)
        for k in range(1, blocks):
            acc = acc + y[k, 64 + u * 32 : 96 + u * 32, :].astype(F32)
        proj[:, u * 128 : (u + 1) * 128] = acc


def final_body(q, state, vv, pack, rest, kg, vg):
    heads, vd, kd = 2, 256, 128
    st = state[...].astype(F32)
    c, s = pack[:, COS : COS + 128], pack[:, SIN : SIN + 128]
    for h in range(heads):
        at = h * 128
        fut = joined(st, h, vd)
        left = pack[:, SCAL + 2 + h : SCAL + 3 + h]
        kt = rest[:, at : at + 128] + left * mmh(vv[h].astype(F32), fut, NT)
        kg[h] = (turned(kt, c, -s) * (kd**-0.5)).astype(BF)
        vt = rest[:, 256 + h * vd : 256 + (h + 1) * vd]
        vg[h] = (vt + left * mmh(pack[:, KR + at : KR + at + 128], fut)).astype(BF)


def a2a(x, axes):
    return lax.all_to_all(x, axes, split_axis=0, concat_axis=0, tiled=True)


def shift(x, by):
    return lax.ppermute(x, TP, [(i, (i + by) % 4) for i in range(4)])


def around(x):
    far = shift(x, 2)
    return x, shift(x, 3), far, shift(x, 1)


def block_rows(k, shape):
    return pl.BlockSpec(shape, lambda i, q, k=k: (lax.rem(q[0] + k, 4), 0))


def block_cols(k, shape):
    return pl.BlockSpec(shape, lambda i, q, k=k: (0, lax.rem(q[0] + k, 4)))


def per_device(
    stream,
    out_grad,
    routes,
    route_weight,
    queries,
    key_vectors,
    value_vectors,
    log_decay,
    out_proj,
    gate_weight,
    up_weight,
    down_weight,
):
    n, width = stream.shape
    quarter = width // 4
    slots = 512
    hidden = gate_weight.shape[2]
    heads, kd = queries.shape[1:]
    vd = value_vectors.shape[2]
    sp = lax.axis_index(SP)
    q = jnp.stack([lax.axis_index(TP), sp // 8, sp % 8, sp]).astype(jnp.int32)
    gate_w, up_w, down_w = gate_weight[0], up_weight[0], down_weight[0]

    own = pl.BlockSpec((n, quarter), lambda i, q: (0, q[0]))
    sent, qt = call(
        "dispatch",
        dispatch_body,
        q,
        (routes.T, route_weight.T, stream, out_grad),
        [((64, 16, quarter), BF), ((2 * n, slots), BF)],
        in_specs={2: own, 3: own},
    )
    came = a2a(sent, SP)
    rows = came[:, :8].reshape(slots, quarter)
    rows_prev, rows_next = shift(rows, 1), shift(rows, 3)
    grads = came[:, 8:].reshape(slots, quarter)
    grads_prev, grads_next = shift(grads, 1), shift(grads, 3)
    rows4 = (rows, rows_next, shift(rows_prev, 1), rows_prev)
    grads4 = (grads, grads_next, shift(grads_next, 3), grads_prev)

    freq = 1.0 / 10000.0 ** jnp.linspace(0.0, 1.0, kd // 2, dtype=F32)
    freq = jnp.repeat(freq, 2)[None, :]
    base = (sp * n).astype(F32) * freq
    angles = jnp.arange(n, dtype=F32)[:, None] * freq
    qv = queries.transpose(1, 0, 2)
    kv = key_vectors.transpose(1, 0, 2)
    vv = value_vectors.transpose(1, 0, 2)
    send, pack = call(
        "prepare",
        prepare_body,
        q,
        (qv, kv, vv, log_decay.T, jnp.cos(base), jnp.sin(base), jnp.cos(angles), jnp.sin(angles)),
        [((64, 16, 128), BF), ((n, 1920), F32)],
        mib=60,
    )
    got = a2a(send, SP)
    state_sent, table = call("prefix", prefix_body, q, (got,), [((64, 8, 128), F32), ((16, 128), F32)])
    state = a2a(state_sent.astype(BF), SP).reshape(slots, 128)
    nbf, back = call(
        "normed", normed_body, q, (state, pack), [((8, n, heads * vd), BF), ((n, 896), F32)]
    )
    nball = a2a(nbf, YC)

    wrow = (quarter, hidden)
    gspec = {k: block_rows(k, wrow) for k in range(4)}
    dspec = {k: block_cols(k, (hidden, quarter)) for k in range(4)}
    act, ga, ua = call(
        "gate_up",
        gate_up_body,
        q,
        (*rows4, *[gate_w] * 4, *[up_w] * 4),
        [((slots, hidden), BF), ((slots, hidden), F32), ((slots, hidden), F32)],
        in_specs={4 + k: s for k, s in gspec.items()} | {8 + k: s for k, s in gspec.items()},
    )
    half = slots // 2
    gp, up, far_lo, far_hi, right_lo, right_hi, left_lo, left_hi, mine = call(
        "expert_back",
        expert_back_body,
        q,
        (*grads4, *[down_w] * 4, *[gate_w] * 4, *[up_w] * 4, ga, ua),
        [((slots, hidden), BF)] * 2 + [((half, quarter), BF)] * 6 + [((slots, quarter), BF)],
        in_specs={4 + k: s for k, s in dspec.items()}
        | {8 + k: s for k, s in gspec.items()}
        | {12 + k: s for k, s in gspec.items()},
        mib=24,
    )
    far_lo, far_hi = shift(far_lo, 1), shift(far_hi, 3)
    right_hi, left_lo = shift(right_hi, 1), shift(left_lo, 3)
    right_lo, left_hi = call(
        "pass_on", pass_on_body, q, (right_lo, far_lo, left_hi, far_hi), [((half, quarter), BF)] * 2
    )
    right_lo, left_hi = shift(right_lo, 1), shift(left_hi, 3)
    gate_grad, up_grad, down_grad, weights_done = call(
        "weight_grads",
        weight_grads_body,
        q,
        (*rows4, *grads4, gp, up, act),
        [((width, hidden), BF), ((width, hidden), BF), ((hidden, width), BF), ((8, 128), F32)],
        out_specs={
            0: pl.BlockSpec(wrow, lambda i, q: (lax.rem(q[0] + i, 4), 0)),
            1: pl.BlockSpec(wrow, lambda i, q: (lax.rem(q[0] + i, 4), 0)),
            2: pl.BlockSpec((hidden, quarter), lambda i, q: (0, lax.rem(q[0] + i, 4))),
        },
        grid=4,
        mib=24,
    )
    (share,) = call(
        "share", share_body, q, (mine, right_lo, right_hi, left_lo, left_hi), [((slots, quarter), BF)]
    )
    share = a2a(share.reshape(64, 8, quarter), SP).reshape(slots, quarter)
    (resid,) = call(
        "combine",
        combine_body,
        q,
        (share, qt, out_grad),
        [((n, quarter), BF)],
        in_specs={2: own},
        after=(weights_done, nball),
    )
    resid4 = around(resid)

    pspec = {4 + k: block_rows(k, (quarter, out_proj.shape[1])) for k in range(4)}
    rg, inner = call(
        "inner_grad",
        inner_grad_body,
        q,
        (*resid4, *[out_proj] * 4, back),
        [((n, heads * vd), F32), ((8, 320, 128), BF)],
        in_specs=pspec,
    )
    inner = a2a(inner, YC)
    qg, rest = call(
        "local_grads",
        local_grads_body,
        q,
        (rg, vv, pack, state),
        [((heads, n, kd), BF), ((n, 768), F32)],
    )
    inside, later = call(
        "plane",
        plane_body,
        q,
        (inner, nball, table),
        [((8, 64, 128), F32), ((8, 192, 128), BF)],
        after=(qg,),
    )
    later = a2a(later, ZAX)
    future, proj_grad = call(
        "planes",
        planes_body,
        q,
        (later, inside, table),
        [((8, 64, 128), BF), ((32, heads * vd), F32)],
    )
    future = a2a(future, YC).reshape(slots, 128)
    kg, vg = call(
        "final",
        final_body,
        q,
        (future, vv, pack, rest),
        [((heads, n, kd), BF), ((heads, n, vd), BF)],
    )
    return (
        gate_grad[None],
        up_grad[None],
        down_grad[None],
        proj_grad,
        qg.transpose(1, 0, 2),
        kg.transpose(1, 0, 2),
        vg.transpose(1, 0, 2),
    )


def solution(mesh):
    split = Mesh(mesh.devices.reshape(8, 4, 2, mesh.shape["tp"]), (*SP, TP))
    placed = (
        P(SP, None),
        P(SP, None),
        P(SP, None),
        P(SP, None),
        P(SP, TP, None),
        P(SP, TP, None),
        P(SP, TP, None),
        P(SP, TP),
        P(None, TP),
        P(SP, None, TP),
        P(SP, None, TP),
        P(SP, TP, None),
    )
    return jax.shard_map(
        per_device,
        mesh=split,
        in_specs=placed,
        out_specs=(
            P(SP, None, TP),
            P(SP, None, TP),
            P(SP, TP, None),
            P(SP, TP),
            P(SP, TP, None),
            P(SP, TP, None),
            P(SP, TP, None),
        ),
        check_vma=False,
    )
```

```python
import jax
import jax.numpy as jnp
from jax import lax
from jax.experimental import pallas as pl
from jax.experimental.pallas import tpu as pltpu
from jax.sharding import Mesh
from jax.sharding import PartitionSpec as P


SP = ("sp_0", "sp_1", "sp_2")
YC = ("sp_1", "sp_2")
ZAX = "sp_0"
TP = "tp"


CLAMP_LIMIT = 7.0
GATE_SLOPE = 1.702
EPSILON = 1e-06
HI = lax.Precision.HIGHEST
F32 = jnp.float32
BF = jnp.bfloat16

NN = (((1,), (0,)), ((), ()))
NT = (((1,), (1,)), ((), ()))
TN = (((0,), (0,)), ((), ()))


def mm(a, b, dims=NN):
    return lax.dot_general(a, b, dims, preferred_element_type=F32)


def mmh(a, b, dims=NN):
    return lax.dot_general(a, b, dims, precision=HI, preferred_element_type=F32)


def iota(shape, dim):
    return lax.broadcasted_iota(jnp.int32, shape, dim)


def whole(shape):
    return pl.BlockSpec(shape, lambda i, q: (0,) * len(shape))


def call(body, q, args, outs, in_specs=None, out_specs=None, grid=1, after=(), mib=16, hbm_in=(), hbm_out=()):
    in_specs = dict(in_specs or {})
    out_specs = out_specs or {}
    used = len(args)
    args = (*args, *after)
    args = tuple(pltpu.with_memory_space_constraint(a, pltpu.HBM) if i in hbm_in else a for i, a in enumerate(args))
    for i in range(used, len(args)):
        in_specs[i] = pl.BlockSpec(memory_space=pltpu.HBM)

    def kernel(q_ref, *refs):
        body(q_ref, *refs[:used], *refs[len(args) :])

    return pl.pallas_call(
        kernel,
        out_shape=[(pltpu.HBM if i in hbm_out else jax.ShapeDtypeStruct)(s, d) for i, (s, d) in enumerate(outs)],
        grid_spec=pltpu.PrefetchScalarGridSpec(
            num_scalar_prefetch=1,
            grid=(grid,),
            in_specs=[in_specs.get(i, whole(a.shape)) for i, a in enumerate(args)],
            out_specs=[out_specs.get(i, whole(s)) for i, (s, _) in enumerate(outs)],
        ),
        compiler_params=pltpu.CompilerParams(vmem_limit_bytes=mib << 20),
    )(q, *args)


def slots_of(routes):
    n = routes.shape[1]
    ti, tj = iota((n, n), 0), iota((n, n), 1)
    eye = ti == tj
    before = ti < tj
    r = routes[...].astype(F32)

    def col(c):
        return jnp.sum(jnp.where(eye, c, 0.0), axis=1, keepdims=True)

    e0r, e1r = r[0:1], r[1:2]
    e0, e1 = col(e0r), col(e1r)

    def earlier(er):
        same = (e0 == er).astype(F32) + (e1 == er).astype(F32)
        return jnp.sum(jnp.where(before, same, 0.0), axis=0, keepdims=True)

    cap = 8
    d0 = e0r * cap + earlier(e0r)
    d1 = e1r * cap + earlier(e1r) + (e0r == e1r).astype(F32)
    return d0, d1, col


def dispatch_body(q, routes, rw, stream, og, send, qt):
    n = routes.shape[1]
    slots = qt.shape[1]
    d0, d1, col = slots_of(routes)
    w = rw[...]
    di = iota((slots, n), 0).astype(F32)
    q0, q1 = di == d0, di == d1
    weight = jnp.where(q0, w[0:1], 0.0) + jnp.where(q1, w[1:2], 0.0)
    weight = jnp.sum(weight, axis=1, keepdims=True)
    pick = (jnp.where(q0, 1.0, 0.0) + jnp.where(q1, 1.0, 0.0)).astype(BF)
    rows = mm(pick, stream[...]).reshape(64, 8, -1)
    grads = (mm(pick, og[...]) * weight).reshape(64, 8, -1)
    send[...] = jnp.concatenate([rows, grads], axis=1).astype(BF)
    dl = iota((n, slots), 1).astype(F32)
    qt[0:n, :] = jnp.where(dl == col(d0), 1.0, 0.0).astype(BF)
    qt[n : 2 * n, :] = jnp.where(dl == col(d1), 1.0, 0.0).astype(BF)


def combine_body(q, ret, qt, og, resid):
    n = og.shape[0]
    back = mm(qt[...], ret[...])
    resid[...] = ((og[...].astype(F32) + back[0:n]) + back[n : 2 * n]).astype(BF)


def gate_up_body(q, r0, r1, r2, r3, g0, g1, g2, g3, u0, u1, u2, u3, act, ga, ua):
    rows = (r0, r1, r2, r3)
    gate = mm(r0[...], g0[...])
    up = mm(r0[...], u0[...])
    for r, g, u in zip(rows[1:], (g1, g2, g3), (u1, u2, u3)):
        x = r[...]
        gate = gate + mm(x, g[...])
        up = up + mm(x, u[...])
    gc = jnp.minimum(gate, CLAMP_LIMIT)
    uc = jnp.clip(up, -CLAMP_LIMIT, CLAMP_LIMIT)
    sig = 1.0 / (1.0 + jnp.exp(-GATE_SLOPE * gc))
    gs = gc * sig
    act[...] = (gs * (uc + 1.0)).astype(BF)
    slope = sig + GATE_SLOPE * gs * (1.0 - sig)
    ga[...] = jnp.where(gate < CLAMP_LIMIT, (uc + 1.0) * slope, 0.0)
    ua[...] = jnp.where(jnp.abs(up) < CLAMP_LIMIT, gs, 0.0)


def expert_back_body(
    q, x0, x1, x2, x3, d0, d1, d2, d3, g0, g1, g2, g3, u0, u1, u2, u3, ga, ua,
    gp, up, far_lo, far_hi, right_lo, right_hi, left_lo, left_hi, mine,
):
    act_grad = mm(x0[...], d0[...], NT)
    for x, d in zip((x1, x2, x3), (d1, d2, d3)):
        act_grad = act_grad + mm(x[...], d[...], NT)
    gpg = (act_grad * ga[...]).astype(BF)
    upg = (act_grad * ua[...]).astype(BF)
    gp[...] = gpg
    up[...] = upg

    def back(g, u):
        return (mm(gpg, g[...], NT) + mm(upg, u[...], NT)).astype(BF)

    half = far_lo.shape[0]
    for lo, hi, part in ((far_lo, far_hi, back(g2, u2)), (right_lo, right_hi, back(g1, u1)), (left_lo, left_hi, back(g3, u3))):
        lo[...] = part[:half]
        hi[...] = part[half:]
    mine[...] = back(g0, u0)


def pass_on_body(q, right_lo, far_lo, left_hi, far_hi, right, left):
    right[...] = (right_lo[...].astype(F32) + far_lo[...].astype(F32)).astype(BF)
    left[...] = (left_hi[...].astype(F32) + far_hi[...].astype(F32)).astype(BF)


def share_body(q, mine, a_lo, a_hi, b_lo, b_hi, out):
    half = a_lo.shape[0]
    m = mine[...].astype(F32)
    out[:half, :] = (m[:half] + (a_lo[...].astype(F32) + b_lo[...].astype(F32))).astype(BF)
    out[half:, :] = (m[half:] + (a_hi[...].astype(F32) + b_hi[...].astype(F32))).astype(BF)


def weight_grads_body(q, r0, r1, r2, r3, x0, x1, x2, x3, gp, up, act, gw, uw, dw, token):
    token[...] = jnp.zeros(token.shape, F32)
    step = pl.program_id(0)
    for k, (r, x) in enumerate(zip((r0, r1, r2, r3), (x0, x1, x2, x3))):

        @pl.when(step == k)
        def _(r=r, x=x):
            rt = r[...]
            gw[...] = mm(rt, gp[...], TN).astype(BF)
            uw[...] = mm(rt, up[...], TN).astype(BF)
            dw[...] = mm(act[...], x[...], TN).astype(BF)


def turned(x, c, s):
    even = (iota(x.shape, 1) % 2) == 0
    n = x.shape[1]
    other = jnp.where(even, -pltpu.roll(x, n - 1, 1), pltpu.roll(x, 1, 1))
    return x * c + other * s


QR, KR, WTS, MASK, SCAL, COS, SIN, INTRA = 0, 256, 512, 768, 1024, 1152, 1280, 1408


def prepare_body(q, qv, kv, vv, ld, cb, sb, cr, sr, send, pack):
    heads, n, kd = qv.shape
    vd = vv.shape[2]
    ti, tj = iota((n, n), 0), iota((n, n), 1)
    eye, causal = ti == tj, ti >= tj
    c = cb[...] * cr[...] - sb[...] * sr[...]
    s = sb[...] * cr[...] + cb[...] * sr[...]
    pack[:, COS : COS + kd] = c
    pack[:, SIN : SIN + kd] = s
    pieces = []
    logs = jnp.zeros((1, 8, 128), F32)
    sub = iota((1, 8, 128), 1)
    scal = jnp.zeros((n, 128), F32)
    lane = iota((n, 128), 1)
    for h in range(heads):
        col = jnp.sum(jnp.where(eye, ld[h : h + 1, :], 0.0), axis=1, keepdims=True)
        rt_r = jnp.sum(jnp.where(ti <= tj, col, 0.0), axis=0, keepdims=True)
        rt_c = jnp.sum(jnp.where(eye, rt_r, 0.0), axis=1, keepdims=True)
        total = rt_r[:, n - 1 : n]
        mask = jnp.where(causal, jnp.exp(jnp.where(causal, rt_c - rt_r, 0.0)), 0.0)
        grow = jnp.exp(rt_c)
        left = jnp.exp(total - rt_c)
        qh = turned(qv[h].astype(F32), c, s)
        kh = turned(kv[h].astype(F32), c, s) * (kd**-0.5)
        vh = vv[h].astype(F32)
        inner = mmh((kh * left).T, vh)
        for u in range(vd // 128):
            pieces.append(inner[:, u * 128 : (u + 1) * 128])
        hi = total.astype(BF).astype(F32)
        mid = (total - hi).astype(BF).astype(F32)
        for k, part in enumerate((hi, mid, total - hi - mid)):
            logs = jnp.where(sub == 3 * h + k, part[None], logs)
        w = mmh(qh, kh, NT) * mask
        pack[:, INTRA + h * vd : INTRA + (h + 1) * vd] = mmh(w, vh)
        at = h * 128
        pack[:, QR + at : QR + at + 128] = qh
        pack[:, KR + at : KR + at + 128] = kh
        pack[:, WTS + at : WTS + at + 128] = w
        pack[:, MASK + at : MASK + at + 128] = mask
        scal = jnp.where(lane == h, grow, jnp.where(lane == 2 + h, left, scal))
    pack[:, SCAL : SCAL + 128] = scal
    state = jnp.concatenate(pieces, axis=0).reshape(-1, 8, 128)
    send[...] = jnp.concatenate([state, jnp.broadcast_to(logs, state.shape)], axis=1).astype(BF)


def prefix_body(q, x, out, table):
    n = x.shape[0]
    z, j = q[1], q[2]
    xf = x[...].astype(F32)
    logs = [xf[:, 8 + 3 * h, :] + xf[:, 9 + 3 * h, :] + xf[:, 10 + 3 * h, :] for h in range(2)]
    mine = jnp.where(z >= 4, logs[1], logs[0])[:, 0:1]
    ti, tj = iota((n, n), 0), iota((n, n), 1)
    after = jnp.where(ti > tj, mine, 0.0)
    seg = mmh(jnp.where(tj < ti, 1.0, 0.0), after)
    w = jnp.where(tj < ti, jnp.exp(seg), 0.0)
    acc = mmh(w, jnp.concatenate([xf[:, k, :] for k in range(8)], axis=1))
    out[...] = jnp.stack([acc[:, k * 128 : (k + 1) * 128] for k in range(8)], axis=1).astype(BF)
    other = jnp.where(j >= 4, logs[1], logs[0])[:, 0:1]
    row = jnp.sum(jnp.where(ti == tj, other, 0.0), axis=0, keepdims=True)
    i, m = iota((16, n), 0), iota((16, n), 1)
    low = jnp.where(i == 8, 8 * z - 1, 8 * z + i)
    a = jnp.where((m > low) & (i < 9), row, 0.0)
    m2, c2 = iota((n, 128), 0), iota((n, 128), 1)
    high = jnp.where(c2 < 16, 8 * z + c2, 8 * (c2 - 16))
    b = jnp.where(m2 < high, 1.0, 0.0)
    decay = jnp.exp(mmh(a, b))
    i, c = iota((16, 128), 0), iota((16, 128), 1)
    used = ((c < 8) & ((i == 8) | (c > i))) | ((c == 8) & (i < 8)) | ((i == 7) & (c >= 16) & (c < 24) & (c - 16 > z))
    table[...] = jnp.where(used, decay, 0.0)


def joined(state, h, vd):
    per = vd // 128
    base = h * per * 128
    return jnp.concatenate([state[base + u * 128 : base + (u + 1) * 128, :] for u in range(per)], axis=1)


INV, QDT = 512, 640


def normed_body(q, state, pack, nbf, back):
    n = pack.shape[0]
    heads, vd = 2, 256
    st = state[...].astype(F32)
    lane = iota((n, 128), 1)
    invs = jnp.zeros((n, 128), F32)
    for h in range(heads):
        sl = slice(h * vd, (h + 1) * vd)
        qh = pack[:, QR + h * 128 : QR + (h + 1) * 128]
        grow = pack[:, SCAL + h : SCAL + h + 1]
        ret = pack[:, INTRA + h * vd : INTRA + (h + 1) * vd] + grow * mmh(qh, joined(st, h, vd))
        iv = lax.rsqrt(jnp.mean(ret * ret, axis=1, keepdims=True) + EPSILON)
        nm = ret * iv
        back[:, sl] = nm
        for k in range(nbf.shape[0]):
            nbf[k, :, sl] = nm.astype(BF)
        invs = jnp.where(lane == h, iv, invs)
        back[:, QDT + h * 128 : QDT + (h + 1) * 128] = (qh * grow).T
    back[:, INV : INV + 128] = invs


def inner_grad_body(q, r0, r1, r2, r3, p0, p1, p2, p3, back, rg, send):
    heads, vd = 2, 256
    ng = mm(r0[...], p0[...])
    for r, p in zip((r1, r2, r3), (p1, p2, p3)):
        ng = ng + mm(r[...], p[...])
    for h in range(heads):
        sl = slice(h * vd, (h + 1) * vd)
        nm, g = back[:, sl], ng[:, sl]
        m = jnp.mean(g * nm, axis=1, keepdims=True)
        grad = back[:, INV + h : INV + h + 1] * (g - nm * m)
        rg[:, sl] = grad
        inner = mmh(back[:, QDT + h * 128 : QDT + (h + 1) * 128], grad)
        for u in range(vd // 128):
            for e in range(2):
                part = inner[e * 64 : (e + 1) * 64, u * 128 : (u + 1) * 128]
                send[h * 4 + u * 2 + e, 0:64, :] = part.astype(BF)
    for k, r in enumerate((r0, r1, r2, r3)):
        block = lax.rem(q[0] + k, 4)
        t = r[...].astype(F32).T.astype(BF)
        for lo in range(2):
            at = pl.multiple_of(64 + (block * 2 + lo) * 32, 32)
            for j in range(8):
                src = lo * 256 + j * 32
                send[j, pl.ds(at, 32), :] = t[src : src + 32, :]


def local_grads_body(q, rg, vv, pack, state, qg, rest):
    heads, vd = 2, 256
    parts = []
    st = state[...].astype(F32)
    c, s = pack[:, COS : COS + 128], pack[:, SIN : SIN + 128]
    for h in range(heads):
        at = h * 128
        grad = rg[:, h * vd : (h + 1) * vd]
        score = mmh(grad, vv[h].astype(F32), NT) * pack[:, MASK + at : MASK + at + 128]
        grow = pack[:, SCAL + h : SCAL + h + 1]
        qp = mmh(score, pack[:, KR + at : KR + at + 128]) + grow * mmh(grad, joined(st, h, vd), NT)
        parts.append(turned(qp, c, -s))
        rest[:, at : at + 128] = mmh(score.T, pack[:, QR + at : QR + at + 128])
        rest[:, 256 + h * vd : 256 + (h + 1) * vd] = mmh(pack[:, WTS + at : WTS + at + 128].T, grad)
    qg[...] = jnp.stack(parts, axis=1).astype(BF)


def plane_body(q, x, nb, table, inside, send):
    blocks = x.shape[0]
    parts = [x[k, 0:64, :].astype(F32) for k in range(blocks)]
    for k in range(blocks):
        acc = jnp.zeros((64, 128), F32)
        for m in range(k + 1, blocks):
            acc = acc + table[k : k + 1, m : m + 1] * parts[m]
        inside[k] = acc
    total = jnp.zeros((64, 128), F32)
    for m in range(blocks):
        total = total + table[8:9, m : m + 1] * parts[m]
    total = total.astype(BF)
    proj = mm(x[0, 64:320, :], nb[0])
    for k in range(1, blocks):
        proj = proj + mm(x[k, 64:320, :], nb[k])
    for k in range(blocks):
        send[k, 0:64, :] = total
        for u in range(4):
            send[k, 64 + u * 32 : 96 + u * 32, :] = proj[k * 32 : (k + 1) * 32, u * 128 : (u + 1) * 128].astype(BF)


def planes_body(q, y, inside, table, out, proj):
    blocks = y.shape[0]
    later = jnp.zeros((64, 128), F32)
    for k in range(blocks):
        later = later + table[7:8, 16 + k : 17 + k] * y[k, 0:64, :].astype(F32)
    for k in range(blocks):
        out[k] = (inside[k] + table[k : k + 1, 8:9] * later).astype(BF)
    for u in range(4):
        acc = y[0, 64 + u * 32 : 96 + u * 32, :].astype(F32)
        for k in range(1, blocks):
            acc = acc + y[k, 64 + u * 32 : 96 + u * 32, :].astype(F32)
        proj[:, u * 128 : (u + 1) * 128] = acc


def final_body(q, state, vv, pack, rest, kg, vg):
    heads, vd, kd = 2, 256, 128
    keys, values = [], []
    st = state[...].astype(F32)
    c, s = pack[:, COS : COS + 128], pack[:, SIN : SIN + 128]
    for h in range(heads):
        at = h * 128
        fut = joined(st, h, vd)
        left = pack[:, SCAL + 2 + h : SCAL + 3 + h]
        kt = rest[:, at : at + 128] + left * mmh(vv[h].astype(F32), fut, NT)
        keys.append(turned(kt, c, -s) * (kd**-0.5))
        vt = rest[:, 256 + h * vd : 256 + (h + 1) * vd]
        values.append(vt + left * mmh(pack[:, KR + at : KR + at + 128], fut))
    kg[...] = jnp.stack(keys, axis=1).astype(BF)
    vg[...] = jnp.stack(values, axis=1).astype(BF)


def a2a(x, axes):
    return lax.all_to_all(x, axes, split_axis=0, concat_axis=0, tiled=True)


def shift(x, by):
    return lax.ppermute(x, TP, [(i, (i + by) % 4) for i in range(4)])


def around(x):
    far = shift(x, 2)
    return x, shift(x, 3), far, shift(x, 1)


def block_rows(k, shape):
    return pl.BlockSpec(shape, lambda i, q, k=k: (lax.rem(q[0] + k, 4), 0))


def block_cols(k, shape):
    return pl.BlockSpec(shape, lambda i, q, k=k: (0, lax.rem(q[0] + k, 4)))


def per_device(
    stream,
    out_grad,
    routes,
    route_weight,
    queries,
    key_vectors,
    value_vectors,
    log_decay,
    out_proj,
    gate_weight,
    up_weight,
    down_weight,
):
    n, width = stream.shape
    quarter = width // 4
    slots = 512
    hidden = gate_weight.shape[2]
    heads, kd = queries.shape[1:]
    vd = value_vectors.shape[2]
    sp = lax.axis_index(SP)
    q = jnp.stack([lax.axis_index(TP), sp // 8, sp % 8, sp]).astype(jnp.int32)
    gate_w, up_w, down_w = gate_weight[0], up_weight[0], down_weight[0]

    own = pl.BlockSpec((n, quarter), lambda i, q: (0, q[0]))
    sent, qt = call(
        dispatch_body,
        q,
        (routes.T, route_weight.T, stream, out_grad),
        [((64, 16, quarter), BF), ((2 * n, slots), BF)],
        in_specs={2: own, 3: own},
        mib=60,
    )
    came = a2a(sent, SP)
    rows = came[:, :8].reshape(slots, quarter)
    grads = came[:, 8:].reshape(slots, quarter)
    rows_prev, rows_next = shift(rows, 1), shift(rows, 3)
    grads_prev, grads_next = shift(grads, 1), shift(grads, 3)
    rows_far, grads_far = shift(rows_prev, 1), shift(grads_next, 3)
    rows4 = (rows, rows_next, rows_far, rows_prev)
    grads4 = (grads, grads_next, grads_far, grads_prev)

    freq = 1.0 / 10000.0 ** jnp.linspace(0.0, 1.0, kd // 2, dtype=F32)
    freq = jnp.repeat(freq, 2)[None, :]
    base = (sp * n).astype(F32) * freq
    angles = jnp.arange(n, dtype=F32)[:, None] * freq
    qv = queries.transpose(1, 0, 2)
    kv = key_vectors.transpose(1, 0, 2)
    vv = value_vectors.transpose(1, 0, 2)
    send, pack = call(
        prepare_body,
        q,
        (qv, kv, vv, log_decay.T, jnp.cos(base), jnp.sin(base), jnp.cos(angles), jnp.sin(angles)),
        [((64, 16, 128), BF), ((n, 1920), F32)],
        mib=60,
    )
    got = a2a(send, SP)
    state_sent, table = call(prefix_body, q, (got,), [((64, 8, 128), BF), ((16, 128), F32)])
    state = a2a(state_sent, SP).reshape(slots, 128)
    nbf, back = call(
        normed_body, q, (state, pack), [((8, n, heads * vd), BF), ((n, 896), F32)],
        hbm_out=(0, 1),
    )
    nball = a2a(nbf, YC)

    wrow = (quarter, hidden)
    gspec = {k: block_rows(k, wrow) for k in range(4)}
    dspec = {k: block_cols(k, (hidden, quarter)) for k in range(4)}
    act, ga, ua = call(
        gate_up_body,
        q,
        (*rows4, *[gate_w] * 4, *[up_w] * 4),
        [((slots, hidden), BF), ((slots, hidden), F32), ((slots, hidden), F32)],
        in_specs={4 + k: s for k, s in gspec.items()} | {8 + k: s for k, s in gspec.items()},
    )
    half = slots // 2
    gp, up, far_lo, far_hi, right_lo, right_hi, left_lo, left_hi, mine = call(
        expert_back_body,
        q,
        (*grads4, *[down_w] * 4, *[gate_w] * 4, *[up_w] * 4, ga, ua),
        [((slots, hidden), BF)] * 2 + [((half, quarter), BF)] * 6 + [((slots, quarter), BF)],
        in_specs={4 + k: s for k, s in dspec.items()}
        | {8 + k: s for k, s in gspec.items()}
        | {12 + k: s for k, s in gspec.items()},
        mib=24,
        hbm_out=range(9),
    )
    far_lo, far_hi = shift(far_lo, 1), shift(far_hi, 3)
    right_hi, left_lo = shift(right_hi, 1), shift(left_lo, 3)
    right_lo, left_hi = call(
        pass_on_body, q, (right_lo, far_lo, left_hi, far_hi), [((half, quarter), BF)] * 2,
        hbm_in=range(4), hbm_out=range(2),
    )
    right_lo, left_hi = shift(right_lo, 1), shift(left_hi, 3)
    gate_grad, up_grad, down_grad, weights_done = call(
        weight_grads_body,
        q,
        (*rows4, *grads4, gp, up, act),
        [((width, hidden), BF), ((width, hidden), BF), ((hidden, width), BF), ((8, 128), F32)],
        out_specs={
            0: pl.BlockSpec(wrow, lambda i, q: (lax.rem(q[0] + i, 4), 0)),
            1: pl.BlockSpec(wrow, lambda i, q: (lax.rem(q[0] + i, 4), 0)),
            2: pl.BlockSpec((hidden, quarter), lambda i, q: (0, lax.rem(q[0] + i, 4))),
        },
        grid=4,
        mib=24,
    )
    (share,) = call(
        share_body, q, (mine, right_lo, right_hi, left_lo, left_hi), [((slots, quarter), BF)],
        hbm_in=range(5),
    )
    share = a2a(share.reshape(64, 8, quarter), SP).reshape(slots, quarter)
    (resid,) = call(
        combine_body,
        q,
        (share, qt, out_grad),
        [((n, quarter), BF)],
        in_specs={2: own},
        after=(weights_done, nball),
        hbm_in=(1, 2),
    )
    resid4 = around(resid)

    pspec = {4 + k: block_rows(k, (quarter, out_proj.shape[1])) for k in range(4)}
    rg, inner = call(
        inner_grad_body,
        q,
        (*resid4, *[out_proj] * 4, back),
        [((n, heads * vd), F32), ((8, 320, 128), BF)],
        in_specs=pspec,
        hbm_in=(8,),
        hbm_out=(0, 1),
    )
    inner = a2a(inner, YC)
    qg, rest = call(local_grads_body, q, (rg, vv, pack, state), [((n, heads, kd), BF), ((n, 768), F32)])
    inside, later = call(plane_body, q, (inner, nball, table), [((8, 64, 128), F32), ((8, 192, 128), BF)], after=(qg,))
    later = a2a(later, ZAX)
    future, proj_grad = call(planes_body, q, (later, inside, table), [((8, 64, 128), BF), ((32, heads * vd), F32)])
    future = a2a(future, YC).reshape(slots, 128)
    kg, vg = call(final_body, q, (future, vv, pack, rest), [((n, heads, kd), BF), ((n, heads, vd), BF)])
    return (
        gate_grad[None],
        up_grad[None],
        down_grad[None],
        proj_grad,
        qg,
        kg,
        vg,
    )


def solution(mesh):
    split = Mesh(mesh.devices.reshape(8, 4, 2, mesh.shape["tp"]), (*SP, TP))
    placed = (
        P(SP, None),
        P(SP, None),
        P(SP, None),
        P(SP, None),
        P(SP, TP, None),
        P(SP, TP, None),
        P(SP, TP, None),
        P(SP, TP),
        P(None, TP),
        P(SP, None, TP),
        P(SP, None, TP),
        P(SP, TP, None),
    )

    return jax.shard_map(
        per_device,
        mesh=split,
        in_specs=placed,
        out_specs=(
            P(SP, None, TP),
            P(SP, None, TP),
            P(SP, TP, None),
            P(SP, TP),
            P(SP, TP, None),
            P(SP, TP, None),
            P(SP, TP, None),
        ),
        check_vma=False,
    )
```

```python
import jax
import jax.numpy as jnp
from jax import lax
from jax.experimental import pallas as pl
from jax.experimental.pallas import tpu as pltpu
from jax.sharding import Mesh
from jax.sharding import PartitionSpec as P


SP = ("sp_0", "sp_1", "sp_2")
YC = ("sp_1", "sp_2")
ZAX = "sp_0"
TP = "tp"


CLAMP_LIMIT = 7.0
GATE_SLOPE = 1.702
EPSILON = 1e-06
HI = lax.Precision.HIGHEST
F32 = jnp.float32
BF = jnp.bfloat16

NN = (((1,), (0,)), ((), ()))
NT = (((1,), (1,)), ((), ()))
TN = (((0,), (0,)), ((), ()))


def mm(a, b, dims=NN):
    return lax.dot_general(a, b, dims, preferred_element_type=F32)


def mmh(a, b, dims=NN):
    return lax.dot_general(a, b, dims, precision=HI, preferred_element_type=F32)


def iota(shape, dim):
    return lax.broadcasted_iota(jnp.int32, shape, dim)


def whole(shape):
    return pl.BlockSpec(shape, lambda i, q: (0,) * len(shape))


def call(body, q, args, outs, in_specs=None, out_specs=None, grid=1, after=(), mib=16, hbm_in=(), hbm_out=()):
    in_specs = dict(in_specs or {})
    out_specs = out_specs or {}
    used = len(args)
    args = (*args, *after)
    args = tuple(pltpu.with_memory_space_constraint(a, pltpu.HBM) if i in hbm_in else a for i, a in enumerate(args))
    for i in range(used, len(args)):
        in_specs[i] = pl.BlockSpec(memory_space=pltpu.HBM)

    def kernel(q_ref, *refs):
        body(q_ref, *refs[:used], *refs[len(args) :])

    return pl.pallas_call(
        kernel,
        out_shape=[(pltpu.HBM if i in hbm_out else jax.ShapeDtypeStruct)(s, d) for i, (s, d) in enumerate(outs)],
        grid_spec=pltpu.PrefetchScalarGridSpec(
            num_scalar_prefetch=1,
            grid=(grid,),
            in_specs=[in_specs.get(i, whole(a.shape)) for i, a in enumerate(args)],
            out_specs=[out_specs.get(i, whole(s)) for i, (s, _) in enumerate(outs)],
        ),
        compiler_params=pltpu.CompilerParams(vmem_limit_bytes=mib << 20),
    )(q, *args)


def slots_of(routes):
    n = routes.shape[1]
    ti, tj = iota((n, n), 0), iota((n, n), 1)
    eye = ti == tj
    before = ti < tj
    r = routes[...].astype(F32)

    def col(c):
        return jnp.sum(jnp.where(eye, c, 0.0), axis=1, keepdims=True)

    e0r, e1r = r[0:1], r[1:2]
    e0, e1 = col(e0r), col(e1r)

    def earlier(er):
        same = (e0 == er).astype(F32) + (e1 == er).astype(F32)
        return jnp.sum(jnp.where(before, same, 0.0), axis=0, keepdims=True)

    cap = 8
    d0 = e0r * cap + earlier(e0r)
    d1 = e1r * cap + earlier(e1r) + (e0r == e1r).astype(F32)
    return d0, d1, col


def dispatch_body(q, routes, rw, stream, og, send, qt):
    n = routes.shape[1]
    slots = qt.shape[1]
    d0, d1, col = slots_of(routes)
    w = rw[...]
    di = iota((slots, n), 0).astype(F32)
    q0, q1 = di == d0, di == d1
    weight = jnp.where(q0, w[0:1], 0.0) + jnp.where(q1, w[1:2], 0.0)
    weight = jnp.sum(weight, axis=1, keepdims=True)
    pick = (jnp.where(q0, 1.0, 0.0) + jnp.where(q1, 1.0, 0.0)).astype(BF)
    rows = mm(pick, stream[...]).reshape(64, 8, -1)
    grads = (mm(pick, og[...]) * weight).reshape(64, 8, -1)
    send[...] = jnp.concatenate([rows, grads], axis=1).astype(BF)
    dl = iota((n, slots), 1).astype(F32)
    qt[0:n, :] = jnp.where(dl == col(d0), 1.0, 0.0).astype(BF)
    qt[n : 2 * n, :] = jnp.where(dl == col(d1), 1.0, 0.0).astype(BF)


def combine_body(q, ret, qt, og, resid):
    n = og.shape[0]
    back = mm(qt[...], ret[...])
    resid[...] = ((og[...].astype(F32) + back[0:n]) + back[n : 2 * n]).astype(BF)


def early_body(q, r0, r1, r3, x0, x1, x3, g0, g1, g3, u0, u1, u3, d0, d1, d3, gate, up, act_grad):
    a, b, c = r0[...], r1[...], r3[...]
    gate[...] = mm(a, g0[...]) + mm(b, g1[...]) + mm(c, g3[...])
    up[...] = mm(a, u0[...]) + mm(b, u1[...]) + mm(c, u3[...])
    act_grad[...] = mm(x0[...], d0[...], NT) + mm(x1[...], d1[...], NT) + mm(x3[...], d3[...], NT)


def expert_back_body(
    q, r2, x2, d2, g0, g1, g2, g3, u0, u1, u2, u3, gate_part, up_part, act_part,
    act, gp, up, far_lo, far_hi, right_lo, right_hi, left_lo, left_hi, mine,
):
    x = r2[...]
    gate = gate_part[...] + mm(x, g2[...])
    upv = up_part[...] + mm(x, u2[...])
    act_grad = act_part[...] + mm(x2[...], d2[...], NT)
    gc = jnp.minimum(gate, CLAMP_LIMIT)
    uc = jnp.clip(upv, -CLAMP_LIMIT, CLAMP_LIMIT)
    sig = 1.0 / (1.0 + jnp.exp(-GATE_SLOPE * gc))
    gs = gc * sig
    act[...] = (gs * (uc + 1.0)).astype(BF)
    slope = sig + GATE_SLOPE * gs * (1.0 - sig)
    gpg = jnp.where(gate < CLAMP_LIMIT, act_grad * (uc + 1.0) * slope, 0.0).astype(BF)
    upg = jnp.where(jnp.abs(upv) < CLAMP_LIMIT, act_grad * gs, 0.0).astype(BF)
    gp[...] = gpg
    up[...] = upg

    def back(g, u):
        return (mm(gpg, g[...], NT) + mm(upg, u[...], NT)).astype(BF)

    half = far_lo.shape[0]
    for lo, hi, part in ((far_lo, far_hi, back(g2, u2)), (right_lo, right_hi, back(g1, u1)), (left_lo, left_hi, back(g3, u3))):
        lo[...] = part[:half]
        hi[...] = part[half:]
    mine[...] = back(g0, u0)


def weight_grads_body(q, r0, r1, r2, r3, x0, x1, x2, x3, gp, up, act, gw, uw, dw):
    step = pl.program_id(0)
    for k, (r, x) in enumerate(zip((r0, r1, r2, r3), (x0, x1, x2, x3))):

        @pl.when(step == k)
        def _(r=r, x=x):
            rt = r[...]
            gw[...] = mm(rt, gp[...], TN).astype(BF)
            uw[...] = mm(rt, up[...], TN).astype(BF)
            dw[...] = mm(act[...], x[...], TN).astype(BF)


def pass_on_body(q, right_lo, far_lo, left_hi, far_hi, right, left):
    right[...] = (right_lo[...].astype(F32) + far_lo[...].astype(F32)).astype(BF)
    left[...] = (left_hi[...].astype(F32) + far_hi[...].astype(F32)).astype(BF)


def share_body(q, mine, a_lo, a_hi, b_lo, b_hi, out):
    half = a_lo.shape[0]
    m = mine[...].astype(F32)
    out[:half, :] = (m[:half] + (a_lo[...].astype(F32) + b_lo[...].astype(F32))).astype(BF)
    out[half:, :] = (m[half:] + (a_hi[...].astype(F32) + b_hi[...].astype(F32))).astype(BF)


def weight_grads_body(q, r0, r1, r2, r3, x0, x1, x2, x3, gp, up, act, gw, uw, dw):
    step = pl.program_id(0)
    for k, (r, x) in enumerate(zip((r0, r1, r2, r3), (x0, x1, x2, x3))):

        @pl.when(step == k)
        def _(r=r, x=x):
            rt = r[...]
            gw[...] = mm(rt, gp[...], TN).astype(BF)
            uw[...] = mm(rt, up[...], TN).astype(BF)
            dw[...] = mm(act[...], x[...], TN).astype(BF)


def turned(x, c, s):
    even = (iota(x.shape, 1) % 2) == 0
    n = x.shape[1]
    other = jnp.where(even, -pltpu.roll(x, n - 1, 1), pltpu.roll(x, 1, 1))
    return x * c + other * s


QR, KR, WTS, MASK, SCAL, COS, SIN, INTRA = 0, 256, 512, 768, 1024, 1152, 1280, 1408


def prepare_body(q, qv, kv, vv, ld, cb, sb, cr, sr, send, pack):
    heads, n, kd = qv.shape
    vd = vv.shape[2]
    ti, tj = iota((n, n), 0), iota((n, n), 1)
    eye, causal = ti == tj, ti >= tj
    c = cb[...] * cr[...] - sb[...] * sr[...]
    s = sb[...] * cr[...] + cb[...] * sr[...]
    pack[:, COS : COS + kd] = c
    pack[:, SIN : SIN + kd] = s
    pieces = []
    logs = jnp.zeros((1, 8, 128), F32)
    sub = iota((1, 8, 128), 1)
    scal = jnp.zeros((n, 128), F32)
    lane = iota((n, 128), 1)
    for h in range(heads):
        col = jnp.sum(jnp.where(eye, ld[h : h + 1, :], 0.0), axis=1, keepdims=True)
        rt_r = jnp.sum(jnp.where(ti <= tj, col, 0.0), axis=0, keepdims=True)
        rt_c = jnp.sum(jnp.where(eye, rt_r, 0.0), axis=1, keepdims=True)
        total = rt_r[:, n - 1 : n]
        mask = jnp.where(causal, jnp.exp(jnp.where(causal, rt_c - rt_r, 0.0)), 0.0)
        grow = jnp.exp(rt_c)
        left = jnp.exp(total - rt_c)
        qh = turned(qv[h].astype(F32), c, s)
        kh = turned(kv[h].astype(F32), c, s) * (kd**-0.5)
        vh = vv[h].astype(F32)
        inner = mmh((kh * left).T, vh)
        for u in range(vd // 128):
            pieces.append(inner[:, u * 128 : (u + 1) * 128])
        hi = total.astype(BF).astype(F32)
        mid = (total - hi).astype(BF).astype(F32)
        for k, part in enumerate((hi, mid, total - hi - mid)):
            logs = jnp.where(sub == 3 * h + k, part[None], logs)
        w = mmh(qh, kh, NT) * mask
        pack[:, INTRA + h * vd : INTRA + (h + 1) * vd] = mmh(w, vh)
        at = h * 128
        pack[:, QR + at : QR + at + 128] = qh
        pack[:, KR + at : KR + at + 128] = kh
        pack[:, WTS + at : WTS + at + 128] = w
        pack[:, MASK + at : MASK + at + 128] = mask
        scal = jnp.where(lane == h, grow, jnp.where(lane == 2 + h, left, scal))
    pack[:, SCAL : SCAL + 128] = scal
    state = jnp.concatenate(pieces, axis=0).reshape(-1, 8, 128)
    send[...] = jnp.concatenate([state, jnp.broadcast_to(logs, state.shape)], axis=1).astype(BF)


def prefix_body(q, x, out, table):
    n = x.shape[0]
    z, j = q[1], q[2]
    xf = x[...].astype(F32)
    logs = [xf[:, 8 + 3 * h, :] + xf[:, 9 + 3 * h, :] + xf[:, 10 + 3 * h, :] for h in range(2)]
    mine = jnp.where(z >= 4, logs[1], logs[0])[:, 0:1]
    ti, tj = iota((n, n), 0), iota((n, n), 1)
    after = jnp.where(ti > tj, mine, 0.0)
    seg = mmh(jnp.where(tj < ti, 1.0, 0.0), after)
    w = jnp.where(tj < ti, jnp.exp(seg), 0.0)
    acc = mmh(w, jnp.concatenate([xf[:, k, :] for k in range(8)], axis=1))
    out[...] = jnp.stack([acc[:, k * 128 : (k + 1) * 128] for k in range(8)], axis=1).astype(BF)
    other = jnp.where(j >= 4, logs[1], logs[0])[:, 0:1]
    row = jnp.sum(jnp.where(ti == tj, other, 0.0), axis=0, keepdims=True)
    i, m = iota((16, n), 0), iota((16, n), 1)
    low = jnp.where(i == 8, 8 * z - 1, 8 * z + i)
    a = jnp.where((m > low) & (i < 9), row, 0.0)
    m2, c2 = iota((n, 128), 0), iota((n, 128), 1)
    high = jnp.where(c2 < 16, 8 * z + c2, 8 * (c2 - 16))
    b = jnp.where(m2 < high, 1.0, 0.0)
    decay = jnp.exp(mmh(a, b))
    i, c = iota((16, 128), 0), iota((16, 128), 1)
    used = ((c < 8) & ((i == 8) | (c > i))) | ((c == 8) & (i < 8)) | ((i == 7) & (c >= 16) & (c < 24) & (c - 16 > z))
    table[...] = jnp.where(used, decay, 0.0)


def joined(state, h, vd):
    per = vd // 128
    base = h * per * 128
    return jnp.concatenate([state[base + u * 128 : base + (u + 1) * 128, :] for u in range(per)], axis=1)


INV, QDT = 512, 640


def normed_body(q, state, pack, nbf, back):
    n = pack.shape[0]
    heads, vd = 2, 256
    st = state[...].astype(F32)
    lane = iota((n, 128), 1)
    invs = jnp.zeros((n, 128), F32)
    for h in range(heads):
        sl = slice(h * vd, (h + 1) * vd)
        qh = pack[:, QR + h * 128 : QR + (h + 1) * 128]
        grow = pack[:, SCAL + h : SCAL + h + 1]
        ret = pack[:, INTRA + h * vd : INTRA + (h + 1) * vd] + grow * mmh(qh, joined(st, h, vd))
        iv = lax.rsqrt(jnp.mean(ret * ret, axis=1, keepdims=True) + EPSILON)
        nm = ret * iv
        back[:, sl] = nm
        nbf[:, sl] = nm.astype(BF)
        invs = jnp.where(lane == h, iv, invs)
        back[:, QDT + h * 128 : QDT + (h + 1) * 128] = (qh * grow).T
    back[:, INV : INV + 128] = invs


def inner_grad_body(q, r0, r1, r2, r3, p0, p1, p2, p3, back, rg, send):
    heads, vd = 2, 256
    ng = mm(r0[...], p0[...])
    for r, p in zip((r1, r2, r3), (p1, p2, p3)):
        ng = ng + mm(r[...], p[...])
    for h in range(heads):
        sl = slice(h * vd, (h + 1) * vd)
        nm, g = back[:, sl], ng[:, sl]
        m = jnp.mean(g * nm, axis=1, keepdims=True)
        grad = back[:, INV + h : INV + h + 1] * (g - nm * m)
        rg[:, sl] = grad
        inner = mmh(back[:, QDT + h * 128 : QDT + (h + 1) * 128], grad)
        for u in range(vd // 128):
            for e in range(2):
                part = inner[e * 64 : (e + 1) * 64, u * 128 : (u + 1) * 128]
                send[h * 4 + u * 2 + e, 0:64, :] = part.astype(BF)
    for k, r in enumerate((r0, r1, r2, r3)):
        block = lax.rem(q[0] + k, 4)
        t = r[...].astype(F32).T.astype(BF)
        for lo in range(2):
            at = pl.multiple_of(64 + (block * 2 + lo) * 32, 32)
            for j in range(8):
                src = lo * 256 + j * 32
                send[j, pl.ds(at, 32), :] = t[src : src + 32, :]


def local_grads_body(q, rg, vv, pack, state, qg, rest):
    heads, vd = 2, 256
    parts = []
    st = state[...].astype(F32)
    c, s = pack[:, COS : COS + 128], pack[:, SIN : SIN + 128]
    for h in range(heads):
        at = h * 128
        grad = rg[:, h * vd : (h + 1) * vd]
        score = mmh(grad, vv[h].astype(F32), NT) * pack[:, MASK + at : MASK + at + 128]
        grow = pack[:, SCAL + h : SCAL + h + 1]
        qp = mmh(score, pack[:, KR + at : KR + at + 128]) + grow * mmh(grad, joined(st, h, vd), NT)
        parts.append(turned(qp, c, -s))
        rest[:, at : at + 128] = mmh(score.T, pack[:, QR + at : QR + at + 128])
        rest[:, 256 + h * vd : 256 + (h + 1) * vd] = mmh(pack[:, WTS + at : WTS + at + 128].T, grad)
    qg[...] = jnp.stack(parts, axis=1).astype(BF)


def plane_body(q, x, n0, n1, n2, n3, m0, m1, m2, m3, table, inside, send):
    blocks = x.shape[0]
    parts = [x[k, 0:64, :].astype(F32) for k in range(blocks)]
    for k in range(blocks):
        acc = jnp.zeros((64, 128), F32)
        for m in range(k + 1, blocks):
            acc = acc + table[k : k + 1, m : m + 1] * parts[m]
        inside[k] = acc
    total = jnp.zeros((64, 128), F32)
    for m in range(blocks):
        total = total + table[8:9, m : m + 1] * parts[m]
    total = total.astype(BF)
    proj = 0.0
    y, core = q[2] // 2, q[2] % 2
    for k, nb in enumerate((n0, n1, n2, n3)):
        proj = proj + mm(x[lax.rem(y + k, 4) * 2 + core, 64:320, :], nb[...])
    for k, nb in enumerate((m0, m1, m2, m3)):
        proj = proj + mm(x[lax.rem(y + k, 4) * 2 + 1 - core, 64:320, :], nb[...])
    for k in range(blocks):
        send[k, 0:64, :] = total
        for u in range(4):
            send[k, 64 + u * 32 : 96 + u * 32, :] = proj[k * 32 : (k + 1) * 32, u * 128 : (u + 1) * 128].astype(BF)


def planes_body(q, y, inside, table, out, proj):
    blocks = y.shape[0]
    later = jnp.zeros((64, 128), F32)
    for k in range(blocks):
        later = later + table[7:8, 16 + k : 17 + k] * y[k, 0:64, :].astype(F32)
    for k in range(blocks):
        out[k] = (inside[k] + table[k : k + 1, 8:9] * later).astype(BF)
    for u in range(4):
        acc = y[0, 64 + u * 32 : 96 + u * 32, :].astype(F32)
        for k in range(1, blocks):
            acc = acc + y[k, 64 + u * 32 : 96 + u * 32, :].astype(F32)
        proj[:, u * 128 : (u + 1) * 128] = acc


def final_body(q, state, vv, pack, rest, kg, vg):
    heads, vd, kd = 2, 256, 128
    keys, values = [], []
    st = state[...].astype(F32)
    c, s = pack[:, COS : COS + 128], pack[:, SIN : SIN + 128]
    for h in range(heads):
        at = h * 128
        fut = joined(st, h, vd)
        left = pack[:, SCAL + 2 + h : SCAL + 3 + h]
        kt = rest[:, at : at + 128] + left * mmh(vv[h].astype(F32), fut, NT)
        keys.append(turned(kt, c, -s) * (kd**-0.5))
        vt = rest[:, 256 + h * vd : 256 + (h + 1) * vd]
        values.append(vt + left * mmh(pack[:, KR + at : KR + at + 128], fut))
    kg[...] = jnp.stack(keys, axis=1).astype(BF)
    vg[...] = jnp.stack(values, axis=1).astype(BF)


def a2a(x, axes):
    return lax.all_to_all(x, axes, split_axis=0, concat_axis=0, tiled=True)


def shift(x, by):
    return lax.ppermute(x, TP, [(i, (i + by) % 4) for i in range(4)])


def around(x):
    far = shift(x, 2)
    return x, shift(x, 3), far, shift(x, 1)


def block_rows(k, shape):
    return pl.BlockSpec(shape, lambda i, q, k=k: (lax.rem(q[0] + k, 4), 0))


def block_cols(k, shape):
    return pl.BlockSpec(shape, lambda i, q, k=k: (0, lax.rem(q[0] + k, 4)))


def per_device(
    stream,
    out_grad,
    routes,
    route_weight,
    queries,
    key_vectors,
    value_vectors,
    log_decay,
    out_proj,
    gate_weight,
    up_weight,
    down_weight,
):
    n, width = stream.shape
    quarter = width // 4
    slots = 512
    hidden = gate_weight.shape[2]
    heads, kd = queries.shape[1:]
    vd = value_vectors.shape[2]
    sp = lax.axis_index(SP)
    q = jnp.stack([lax.axis_index(TP), sp // 8, sp % 8, sp]).astype(jnp.int32)
    gate_w, up_w, down_w = gate_weight[0], up_weight[0], down_weight[0]

    own = pl.BlockSpec((n, quarter), lambda i, q: (0, q[0]))
    sent, qt = call(
        dispatch_body,
        q,
        (routes.T, route_weight.T, stream, out_grad),
        [((64, 16, quarter), BF), ((2 * n, slots), BF)],
        in_specs={2: own, 3: own},
        mib=60,
    )
    came = a2a(sent, SP)
    rows = came[:, :8].reshape(slots, quarter)
    grads = came[:, 8:].reshape(slots, quarter)
    rows_prev, rows_next = shift(rows, 1), shift(rows, 3)
    grads_prev, grads_next = shift(grads, 1), shift(grads, 3)
    rows_far, grads_far = shift(rows_prev, 1), shift(grads_next, 3)
    rows4 = (rows, rows_next, rows_far, rows_prev)
    grads4 = (grads, grads_next, grads_far, grads_prev)

    freq = 1.0 / 10000.0 ** jnp.linspace(0.0, 1.0, kd // 2, dtype=F32)
    freq = jnp.repeat(freq, 2)[None, :]
    base = (sp * n).astype(F32) * freq
    angles = jnp.arange(n, dtype=F32)[:, None] * freq
    qv = queries.transpose(1, 0, 2)
    kv = key_vectors.transpose(1, 0, 2)
    vv = value_vectors.transpose(1, 0, 2)
    send, pack = call(
        prepare_body,
        q,
        (qv, kv, vv, log_decay.T, jnp.cos(base), jnp.sin(base), jnp.cos(angles), jnp.sin(angles)),
        [((64, 16, 128), BF), ((n, 1920), F32)],
        mib=60,
    )
    got = a2a(send, SP)
    state_sent, table = call(prefix_body, q, (got,), [((64, 8, 128), BF), ((16, 128), F32)])
    state = a2a(state_sent, SP).reshape(slots, 128)
    nbf, back = call(
        normed_body, q, (state, pack), [((n, heads * vd), BF), ((n, 896), F32)],
        hbm_out=(0, 1),
    )
    along = [nbf] + [lax.ppermute(nbf, "sp_1", [(i, (i + by) % 4) for i in range(4)]) for by in (3, 2, 1)]
    nball = along + [lax.ppermute(a, "sp_2", [(0, 1), (1, 0)]) for a in along]

    wrow = (quarter, hidden)
    gspec = {k: block_rows(k, wrow) for k in range(4)}
    dspec = {k: block_cols(k, (hidden, quarter)) for k in range(4)}
    near = (0, 1, 3)
    parts = call(
        early_body,
        q,
        (*[rows4[k] for k in near], *[grads4[k] for k in near], *[gate_w] * 3, *[up_w] * 3, *[down_w] * 3),
        [((slots, hidden), F32)] * 3,
        in_specs={6 + i: gspec[k] for i, k in enumerate(near)}
        | {9 + i: gspec[k] for i, k in enumerate(near)}
        | {12 + i: dspec[k] for i, k in enumerate(near)},
        mib=20,
    )
    half = slots // 2
    act, gp, up, far_lo, far_hi, right_lo, right_hi, left_lo, left_hi, mine = call(
        expert_back_body,
        q,
        (rows4[2], grads4[2], down_w, *[gate_w] * 4, *[up_w] * 4, *parts),
        [((slots, hidden), BF)] * 3 + [((half, quarter), BF)] * 6 + [((slots, quarter), BF)],
        in_specs={2: dspec[2]} | {3 + k: s for k, s in gspec.items()} | {7 + k: s for k, s in gspec.items()},
        mib=24,
        hbm_out=range(10),
    )
    far_lo, far_hi = shift(far_lo, 1), shift(far_hi, 3)
    right_hi, left_lo = shift(right_hi, 1), shift(left_lo, 3)
    right_lo, left_hi = call(
        pass_on_body, q, (right_lo, far_lo, left_hi, far_hi), [((half, quarter), BF)] * 2,
        hbm_in=range(4), hbm_out=range(2),
    )
    right_lo, left_hi = shift(right_lo, 1), shift(left_hi, 3)
    gate_grad, up_grad, down_grad = call(
        weight_grads_body,
        q,
        (*rows4, *grads4, gp, up, act),
        [((width, hidden), BF), ((width, hidden), BF), ((hidden, width), BF)],
        out_specs={
            0: pl.BlockSpec(wrow, lambda i, q: (lax.rem(q[0] + i, 4), 0)),
            1: pl.BlockSpec(wrow, lambda i, q: (lax.rem(q[0] + i, 4), 0)),
            2: pl.BlockSpec((hidden, quarter), lambda i, q: (0, lax.rem(q[0] + i, 4))),
        },
        grid=4,
        mib=24,
    )
    (share,) = call(
        share_body, q, (mine, right_lo, right_hi, left_lo, left_hi), [((slots, quarter), BF)],
        hbm_in=range(5),
    )
    share = a2a(share.reshape(64, 8, quarter), SP).reshape(slots, quarter)
    (resid,) = call(combine_body, q, (share, qt, out_grad), [((n, quarter), BF)], in_specs={2: own}, hbm_in=(1, 2))
    resid4 = around(resid)

    pspec = {4 + k: block_rows(k, (quarter, out_proj.shape[1])) for k in range(4)}
    rg, inner = call(
        inner_grad_body,
        q,
        (*resid4, *[out_proj] * 4, back),
        [((n, heads * vd), F32), ((8, 320, 128), BF)],
        in_specs=pspec,
        hbm_in=(8,),
        hbm_out=(0, 1),
    )
    inner = a2a(inner, YC)
    qg, rest = call(local_grads_body, q, (rg, vv, pack, state), [((n, heads, kd), BF), ((n, 768), F32)])
    inside, later = call(
        plane_body, q, (inner, *nball, table), [((8, 64, 128), F32), ((8, 192, 128), BF)], hbm_in=range(1, 9)
    )
    later = a2a(later, ZAX)
    future, proj_grad = call(planes_body, q, (later, inside, table), [((8, 64, 128), BF), ((32, heads * vd), F32)])
    future = a2a(future, YC).reshape(slots, 128)
    kg, vg = call(final_body, q, (future, vv, pack, rest), [((n, heads, kd), BF), ((n, heads, vd), BF)])
    return (
        gate_grad[None],
        up_grad[None],
        down_grad[None],
        proj_grad,
        qg,
        kg,
        vg,
    )


def solution(mesh):
    split = Mesh(mesh.devices.reshape(8, 4, 2, mesh.shape["tp"]), (*SP, TP))
    placed = (
        P(SP, None),
        P(SP, None),
        P(SP, None),
        P(SP, None),
        P(SP, TP, None),
        P(SP, TP, None),
        P(SP, TP, None),
        P(SP, TP),
        P(None, TP),
        P(SP, None, TP),
        P(SP, None, TP),
        P(SP, TP, None),
    )

    return jax.shard_map(
        per_device,
        mesh=split,
        in_specs=placed,
        out_specs=(
            P(SP, None, TP),
            P(SP, None, TP),
            P(SP, TP, None),
            P(SP, TP),
            P(SP, TP, None),
            P(SP, TP, None),
            P(SP, TP, None),
        ),
        check_vma=False,
    )
```

```python
import jax
import jax.numpy as jnp
from jax import lax
from jax.experimental import pallas as pl
from jax.experimental.pallas import tpu as pltpu
from jax.sharding import Mesh
from jax.sharding import PartitionSpec as P


SP = ("sp_0", "sp_1", "sp_2")
YC = ("sp_1", "sp_2")
ZAX = "sp_0"
TP = "tp"


CLAMP_LIMIT = 7.0
GATE_SLOPE = 1.702
EPSILON = 1e-06
HI = lax.Precision.HIGHEST
F32 = jnp.float32
BF = jnp.bfloat16

NN = (((1,), (0,)), ((), ()))
NT = (((1,), (1,)), ((), ()))
TN = (((0,), (0,)), ((), ()))


def mm(a, b, dims=NN):
    return lax.dot_general(a, b, dims, preferred_element_type=F32)


def mmh(a, b, dims=NN):
    return lax.dot_general(a, b, dims, precision=HI, preferred_element_type=F32)


def iota(shape, dim):
    return lax.broadcasted_iota(jnp.int32, shape, dim)


def whole(shape):
    return pl.BlockSpec(shape, lambda i, q: (0,) * len(shape))


def call(body, q, args, outs, in_specs=None, out_specs=None, grid=1, after=(), mib=16, hbm_in=(), hbm_out=()):
    in_specs = dict(in_specs or {})
    out_specs = out_specs or {}
    used = len(args)
    args = (*args, *after)
    args = tuple(pltpu.with_memory_space_constraint(a, pltpu.HBM) if i in hbm_in else a for i, a in enumerate(args))
    for i in range(used, len(args)):
        in_specs[i] = pl.BlockSpec(memory_space=pltpu.HBM)

    def kernel(q_ref, *refs):
        body(q_ref, *refs[:used], *refs[len(args) :])

    return pl.pallas_call(
        kernel,
        out_shape=[(pltpu.HBM if i in hbm_out else jax.ShapeDtypeStruct)(s, d) for i, (s, d) in enumerate(outs)],
        grid_spec=pltpu.PrefetchScalarGridSpec(
            num_scalar_prefetch=1,
            grid=(grid,),
            in_specs=[in_specs.get(i, whole(a.shape)) for i, a in enumerate(args)],
            out_specs=[out_specs.get(i, whole(s)) for i, (s, _) in enumerate(outs)],
        ),
        compiler_params=pltpu.CompilerParams(vmem_limit_bytes=mib << 20),
    )(q, *args)


def slots_of(routes):
    n = routes.shape[1]
    ti, tj = iota((n, n), 0), iota((n, n), 1)
    eye = ti == tj
    before = ti < tj
    r = routes[...].astype(F32)

    def col(c):
        return jnp.sum(jnp.where(eye, c, 0.0), axis=1, keepdims=True)

    e0r, e1r = r[0:1], r[1:2]
    e0, e1 = col(e0r), col(e1r)

    def earlier(er):
        same = (e0 == er).astype(F32) + (e1 == er).astype(F32)
        return jnp.sum(jnp.where(before, same, 0.0), axis=0, keepdims=True)

    cap = 8
    d0 = e0r * cap + earlier(e0r)
    d1 = e1r * cap + earlier(e1r) + (e0r == e1r).astype(F32)
    return d0, d1, col


def dispatch_body(q, routes, rw, stream, og, send):
    n = routes.shape[1]
    slots = send.shape[0] * 8
    d0, d1, _ = slots_of(routes)
    w = rw[...]
    di = iota((slots, n), 0).astype(F32)
    q0, q1 = di == d0, di == d1
    weight = jnp.where(q0, w[0:1], 0.0) + jnp.where(q1, w[1:2], 0.0)
    weight = jnp.sum(weight, axis=1, keepdims=True)
    pick = (jnp.where(q0, 1.0, 0.0) + jnp.where(q1, 1.0, 0.0)).astype(BF)
    rows = mm(pick, stream[...]).reshape(64, 8, -1)
    grads = (mm(pick, og[...]) * weight).reshape(64, 8, -1)
    send[...] = jnp.concatenate([rows, grads], axis=1).astype(BF)


def back_picks_body(q, routes, qt):
    n, slots = routes.shape[1], qt.shape[1]
    d0, d1, col = slots_of(routes)
    dl = iota((n, slots), 1).astype(F32)
    qt[0:n, :] = jnp.where(dl == col(d0), 1.0, 0.0).astype(BF)
    qt[n : 2 * n, :] = jnp.where(dl == col(d1), 1.0, 0.0).astype(BF)


def combine_body(q, ret, qt, og, resid):
    n = og.shape[0]
    back = mm(qt[...], ret[...])
    resid[...] = ((og[...].astype(F32) + back[0:n]) + back[n : 2 * n]).astype(BF)


def early_body(q, r0, r1, r3, x0, x1, x3, g0, g1, g3, u0, u1, u3, d0, d1, d3, gate, up, act_grad):
    a, b, c = r0[...], r1[...], r3[...]
    gate[...] = mm(a, g0[...]) + mm(b, g1[...]) + mm(c, g3[...])
    up[...] = mm(a, u0[...]) + mm(b, u1[...]) + mm(c, u3[...])
    act_grad[...] = mm(x0[...], d0[...], NT) + mm(x1[...], d1[...], NT) + mm(x3[...], d3[...], NT)


def hidden_grads_body(q, r2, x2, d2, g2, u2, gate_part, up_part, act_part, act, gp, up, far_lo, far_hi):
    x = r2[...]
    gate = gate_part[...] + mm(x, g2[...])
    upv = up_part[...] + mm(x, u2[...])
    act_grad = act_part[...] + mm(x2[...], d2[...], NT)
    gc = jnp.minimum(gate, CLAMP_LIMIT)
    uc = jnp.clip(upv, -CLAMP_LIMIT, CLAMP_LIMIT)
    sig = 1.0 / (1.0 + jnp.exp(-GATE_SLOPE * gc))
    gs = gc * sig
    act[...] = (gs * (uc + 1.0)).astype(BF)
    slope = sig + GATE_SLOPE * gs * (1.0 - sig)
    gpg = jnp.where(gate < CLAMP_LIMIT, act_grad * (uc + 1.0) * slope, 0.0).astype(BF)
    upg = jnp.where(jnp.abs(upv) < CLAMP_LIMIT, act_grad * gs, 0.0).astype(BF)
    gp[...] = gpg
    up[...] = upg
    half = far_lo.shape[0]
    part = (mm(gpg, g2[...], NT) + mm(upg, u2[...], NT)).astype(BF)
    far_lo[...] = part[:half]
    far_hi[...] = part[half:]


def expert_back_body(q, gp, up, g0, g1, g3, u0, u1, u3, right_lo, right_hi, left_lo, left_hi, mine):
    gpg, upg = gp[...], up[...]

    def back(g, u):
        return (mm(gpg, g[...], NT) + mm(upg, u[...], NT)).astype(BF)

    half = right_lo.shape[0]
    for lo, hi, part in ((right_lo, right_hi, back(g1, u1)), (left_lo, left_hi, back(g3, u3))):
        lo[...] = part[:half]
        hi[...] = part[half:]
    mine[...] = back(g0, u0)


def weight_grads_body(q, r0, r1, r2, r3, x0, x1, x2, x3, gp, up, act, gw, uw, dw):
    step = pl.program_id(0)
    for k, (r, x) in enumerate(zip((r0, r1, r2, r3), (x0, x1, x2, x3))):

        @pl.when(step == k)
        def _(r=r, x=x):
            rt = r[...]
            gw[...] = mm(rt, gp[...], TN).astype(BF)
            uw[...] = mm(rt, up[...], TN).astype(BF)
            dw[...] = mm(act[...], x[...], TN).astype(BF)


def pass_on_body(q, right_lo, far_lo, left_hi, far_hi, right, left):
    right[...] = (right_lo[...].astype(F32) + far_lo[...].astype(F32)).astype(BF)
    left[...] = (left_hi[...].astype(F32) + far_hi[...].astype(F32)).astype(BF)


def share_body(q, mine, a_lo, a_hi, b_lo, b_hi, out):
    half = a_lo.shape[0]
    m = mine[...].astype(F32)
    out[:half, :] = (m[:half] + (a_lo[...].astype(F32) + b_lo[...].astype(F32))).astype(BF)
    out[half:, :] = (m[half:] + (a_hi[...].astype(F32) + b_hi[...].astype(F32))).astype(BF)


def weight_grads_body(q, r0, r1, r2, r3, x0, x1, x2, x3, gp, up, act, gw, uw, dw):
    step = pl.program_id(0)
    for k, (r, x) in enumerate(zip((r0, r1, r2, r3), (x0, x1, x2, x3))):

        @pl.when(step == k)
        def _(r=r, x=x):
            rt = r[...]
            gw[...] = mm(rt, gp[...], TN).astype(BF)
            uw[...] = mm(rt, up[...], TN).astype(BF)
            dw[...] = mm(act[...], x[...], TN).astype(BF)


def turned(x, c, s):
    even = (iota(x.shape, 1) % 2) == 0
    n = x.shape[1]
    other = jnp.where(even, -pltpu.roll(x, n - 1, 1), pltpu.roll(x, 1, 1))
    return x * c + other * s


QR, KR, WTS, MASK, SCAL, COS, SIN, INTRA = 0, 256, 512, 768, 1024, 1152, 1280, 1408


def prepare_body(q, qv, kv, vv, ld, cb, sb, cr, sr, send, pack):
    heads, n, kd = qv.shape
    vd = vv.shape[2]
    ti, tj = iota((n, n), 0), iota((n, n), 1)
    eye, causal = ti == tj, ti >= tj
    c = cb[...] * cr[...] - sb[...] * sr[...]
    s = sb[...] * cr[...] + cb[...] * sr[...]
    pack[:, COS : COS + kd] = c
    pack[:, SIN : SIN + kd] = s
    pieces = []
    logs = jnp.zeros((1, 8, 128), F32)
    sub = iota((1, 8, 128), 1)
    scal = jnp.zeros((n, 128), F32)
    lane = iota((n, 128), 1)
    for h in range(heads):
        col = jnp.sum(jnp.where(eye, ld[h : h + 1, :], 0.0), axis=1, keepdims=True)
        rt_r = jnp.sum(jnp.where(ti <= tj, col, 0.0), axis=0, keepdims=True)
        rt_c = jnp.sum(jnp.where(eye, rt_r, 0.0), axis=1, keepdims=True)
        total = rt_r[:, n - 1 : n]
        mask = jnp.where(causal, jnp.exp(jnp.where(causal, rt_c - rt_r, 0.0)), 0.0)
        grow = jnp.exp(rt_c)
        left = jnp.exp(total - rt_c)
        qh = turned(qv[h].astype(F32), c, s)
        kh = turned(kv[h].astype(F32), c, s) * (kd**-0.5)
        vh = vv[h].astype(F32)
        inner = mmh((kh * left).T, vh)
        for u in range(vd // 128):
            pieces.append(inner[:, u * 128 : (u + 1) * 128])
        hi = total.astype(BF).astype(F32)
        mid = (total - hi).astype(BF).astype(F32)
        for k, part in enumerate((hi, mid, total - hi - mid)):
            logs = jnp.where(sub == 3 * h + k, part[None], logs)
        w = mmh(qh, kh, NT) * mask
        pack[:, INTRA + h * vd : INTRA + (h + 1) * vd] = mmh(w, vh)
        at = h * 128
        pack[:, QR + at : QR + at + 128] = qh
        pack[:, KR + at : KR + at + 128] = kh
        pack[:, WTS + at : WTS + at + 128] = w
        pack[:, MASK + at : MASK + at + 128] = mask
        scal = jnp.where(lane == h, grow, jnp.where(lane == 2 + h, left, scal))
    pack[:, SCAL : SCAL + 128] = scal
    state = jnp.concatenate(pieces, axis=0).reshape(-1, 8, 128)
    send[...] = jnp.concatenate([state, jnp.broadcast_to(logs, state.shape)], axis=1).astype(BF)


def prefix_body(q, x, out, table):
    n = x.shape[0]
    z, j = q[1], q[2]
    xf = x[...].astype(F32)
    logs = [xf[:, 8 + 3 * h, :] + xf[:, 9 + 3 * h, :] + xf[:, 10 + 3 * h, :] for h in range(2)]
    mine = jnp.where(z >= 4, logs[1], logs[0])[:, 0:1]
    ti, tj = iota((n, n), 0), iota((n, n), 1)
    after = jnp.where(ti > tj, mine, 0.0)
    seg = mmh(jnp.where(tj < ti, 1.0, 0.0), after)
    w = jnp.where(tj < ti, jnp.exp(seg), 0.0)
    acc = mmh(w, jnp.concatenate([xf[:, k, :] for k in range(8)], axis=1))
    out[...] = jnp.stack([acc[:, k * 128 : (k + 1) * 128] for k in range(8)], axis=1).astype(BF)
    other = jnp.where(j >= 4, logs[1], logs[0])[:, 0:1]
    row = jnp.sum(jnp.where(ti == tj, other, 0.0), axis=0, keepdims=True)
    i, m = iota((16, n), 0), iota((16, n), 1)
    low = jnp.where(i == 8, 8 * z - 1, 8 * z + i)
    a = jnp.where((m > low) & (i < 9), row, 0.0)
    m2, c2 = iota((n, 128), 0), iota((n, 128), 1)
    high = jnp.where(c2 < 16, 8 * z + c2, 8 * (c2 - 16))
    b = jnp.where(m2 < high, 1.0, 0.0)
    decay = jnp.exp(mmh(a, b))
    i, c = iota((16, 128), 0), iota((16, 128), 1)
    used = ((c < 8) & ((i == 8) | (c > i))) | ((c == 8) & (i < 8)) | ((i == 7) & (c >= 16) & (c < 24) & (c - 16 > z))
    table[...] = jnp.where(used, decay, 0.0)


def joined(state, h, vd):
    per = vd // 128
    base = h * per * 128
    return jnp.concatenate([state[base + u * 128 : base + (u + 1) * 128, :] for u in range(per)], axis=1)


INV, QDT = 512, 640


def normed_body(q, state, pack, nbf, back):
    n = pack.shape[0]
    heads, vd = 2, 256
    st = state[...].astype(F32)
    lane = iota((n, 128), 1)
    invs = jnp.zeros((n, 128), F32)
    for h in range(heads):
        sl = slice(h * vd, (h + 1) * vd)
        qh = pack[:, QR + h * 128 : QR + (h + 1) * 128]
        grow = pack[:, SCAL + h : SCAL + h + 1]
        ret = pack[:, INTRA + h * vd : INTRA + (h + 1) * vd] + grow * mmh(qh, joined(st, h, vd))
        iv = lax.rsqrt(jnp.mean(ret * ret, axis=1, keepdims=True) + EPSILON)
        nm = ret * iv
        back[:, sl] = nm
        nbf[:, sl] = nm.astype(BF)
        invs = jnp.where(lane == h, iv, invs)
        back[:, QDT + h * 128 : QDT + (h + 1) * 128] = (qh * grow).T
    back[:, INV : INV + 128] = invs


def inner_grad_body(q, r0, r1, r2, r3, p0, p1, p2, p3, back, rg, send):
    heads, vd = 2, 256
    ng = mm(r0[...], p0[...])
    for r, p in zip((r1, r2, r3), (p1, p2, p3)):
        ng = ng + mm(r[...], p[...])
    for h in range(heads):
        sl = slice(h * vd, (h + 1) * vd)
        nm, g = back[:, sl], ng[:, sl]
        m = jnp.mean(g * nm, axis=1, keepdims=True)
        grad = back[:, INV + h : INV + h + 1] * (g - nm * m)
        rg[:, sl] = grad
        inner = mmh(back[:, QDT + h * 128 : QDT + (h + 1) * 128], grad)
        for u in range(vd // 128):
            for e in range(2):
                part = inner[e * 64 : (e + 1) * 64, u * 128 : (u + 1) * 128]
                send[h * 4 + u * 2 + e, 0:64, :] = part.astype(BF)
    for k, r in enumerate((r0, r1, r2, r3)):
        block = lax.rem(q[0] + k, 4)
        t = r[...].astype(F32).T.astype(BF)
        for lo in range(2):
            at = pl.multiple_of(64 + (block * 2 + lo) * 32, 32)
            for j in range(8):
                src = lo * 256 + j * 32
                send[j, pl.ds(at, 32), :] = t[src : src + 32, :]


def local_grads_body(q, rg, vv, pack, state, qg, rest):
    heads, vd = 2, 256
    parts = []
    st = state[...].astype(F32)
    c, s = pack[:, COS : COS + 128], pack[:, SIN : SIN + 128]
    for h in range(heads):
        at = h * 128
        grad = rg[:, h * vd : (h + 1) * vd]
        score = mmh(grad, vv[h].astype(F32), NT) * pack[:, MASK + at : MASK + at + 128]
        grow = pack[:, SCAL + h : SCAL + h + 1]
        qp = mmh(score, pack[:, KR + at : KR + at + 128]) + grow * mmh(grad, joined(st, h, vd), NT)
        parts.append(turned(qp, c, -s))
        rest[:, at : at + 128] = mmh(score.T, pack[:, QR + at : QR + at + 128])
        rest[:, 256 + h * vd : 256 + (h + 1) * vd] = mmh(pack[:, WTS + at : WTS + at + 128].T, grad)
    qg[...] = jnp.stack(parts, axis=1).astype(BF)


def plane_body(q, x, n0, n1, n2, n3, m0, m1, m2, m3, table, inside, send):
    blocks = x.shape[0]
    parts = [x[k, 0:64, :].astype(F32) for k in range(blocks)]
    for k in range(blocks):
        acc = jnp.zeros((64, 128), F32)
        for m in range(k + 1, blocks):
            acc = acc + table[k : k + 1, m : m + 1] * parts[m]
        inside[k] = acc
    total = jnp.zeros((64, 128), F32)
    for m in range(blocks):
        total = total + table[8:9, m : m + 1] * parts[m]
    total = total.astype(BF)
    proj = 0.0
    y, core = q[2] // 2, q[2] % 2
    for k, nb in enumerate((n0, n1, n2, n3)):
        proj = proj + mm(x[lax.rem(y + k, 4) * 2 + core, 64:320, :], nb[...])
    for k, nb in enumerate((m0, m1, m2, m3)):
        proj = proj + mm(x[lax.rem(y + k, 4) * 2 + 1 - core, 64:320, :], nb[...])
    for k in range(blocks):
        send[k, 0:64, :] = total
        for u in range(4):
            send[k, 64 + u * 32 : 96 + u * 32, :] = proj[k * 32 : (k + 1) * 32, u * 128 : (u + 1) * 128].astype(BF)


def planes_body(q, y, inside, table, out, proj):
    blocks = y.shape[0]
    later = jnp.zeros((64, 128), F32)
    for k in range(blocks):
        later = later + table[7:8, 16 + k : 17 + k] * y[k, 0:64, :].astype(F32)
    for k in range(blocks):
        out[k] = (inside[k] + table[k : k + 1, 8:9] * later).astype(BF)
    for u in range(4):
        acc = y[0, 64 + u * 32 : 96 + u * 32, :].astype(F32)
        for k in range(1, blocks):
            acc = acc + y[k, 64 + u * 32 : 96 + u * 32, :].astype(F32)
        proj[:, u * 128 : (u + 1) * 128] = acc


def final_body(q, state, vv, pack, rest, kg, vg):
    heads, vd, kd = 2, 256, 128
    keys, values = [], []
    st = state[...].astype(F32)
    c, s = pack[:, COS : COS + 128], pack[:, SIN : SIN + 128]
    for h in range(heads):
        at = h * 128
        fut = joined(st, h, vd)
        left = pack[:, SCAL + 2 + h : SCAL + 3 + h]
        kt = rest[:, at : at + 128] + left * mmh(vv[h].astype(F32), fut, NT)
        keys.append(turned(kt, c, -s) * (kd**-0.5))
        vt = rest[:, 256 + h * vd : 256 + (h + 1) * vd]
        values.append(vt + left * mmh(pack[:, KR + at : KR + at + 128], fut))
    kg[...] = jnp.stack(keys, axis=1).astype(BF)
    vg[...] = jnp.stack(values, axis=1).astype(BF)


def a2a(x, axes):
    return lax.all_to_all(x, axes, split_axis=0, concat_axis=0, tiled=True)


def shift(x, by):
    return lax.ppermute(x, TP, [(i, (i + by) % 4) for i in range(4)])


def around(x):
    far = shift(x, 2)
    return x, shift(x, 3), far, shift(x, 1)


def block_rows(k, shape):
    return pl.BlockSpec(shape, lambda i, q, k=k: (lax.rem(q[0] + k, 4), 0))


def block_cols(k, shape):
    return pl.BlockSpec(shape, lambda i, q, k=k: (0, lax.rem(q[0] + k, 4)))


def per_device(
    stream,
    out_grad,
    routes,
    route_weight,
    queries,
    key_vectors,
    value_vectors,
    log_decay,
    out_proj,
    gate_weight,
    up_weight,
    down_weight,
):
    n, width = stream.shape
    quarter = width // 4
    slots = 512
    hidden = gate_weight.shape[2]
    heads, kd = queries.shape[1:]
    vd = value_vectors.shape[2]
    sp = lax.axis_index(SP)
    q = jnp.stack([lax.axis_index(TP), sp // 8, sp % 8, sp]).astype(jnp.int32)
    gate_w, up_w, down_w = gate_weight[0], up_weight[0], down_weight[0]

    own = pl.BlockSpec((n, quarter), lambda i, q: (0, q[0]))
    (sent,) = call(
        dispatch_body,
        q,
        (routes.T, route_weight.T, stream, out_grad),
        [((64, 16, quarter), BF)],
        in_specs={2: own, 3: own},
        mib=60,
    )
    came = a2a(sent, SP)
    rows = came[:, :8].reshape(slots, quarter)
    grads = came[:, 8:].reshape(slots, quarter)
    rows_prev, rows_next = shift(rows, 1), shift(rows, 3)
    grads_prev, grads_next = shift(grads, 1), shift(grads, 3)
    rows_far, grads_far = shift(rows_prev, 1), shift(grads_next, 3)
    rows4 = (rows, rows_next, rows_far, rows_prev)
    grads4 = (grads, grads_next, grads_far, grads_prev)

    freq = 1.0 / 10000.0 ** jnp.linspace(0.0, 1.0, kd // 2, dtype=F32)
    freq = jnp.repeat(freq, 2)[None, :]
    base = (sp * n).astype(F32) * freq
    angles = jnp.arange(n, dtype=F32)[:, None] * freq
    qv = queries.transpose(1, 0, 2)
    kv = key_vectors.transpose(1, 0, 2)
    vv = value_vectors.transpose(1, 0, 2)
    (qt,) = call(back_picks_body, q, (routes.T,), [((2 * n, slots), BF)], hbm_out=(0,))
    send, pack = call(
        prepare_body,
        q,
        (qv, kv, vv, log_decay.T, jnp.cos(base), jnp.sin(base), jnp.cos(angles), jnp.sin(angles)),
        [((64, 16, 128), BF), ((n, 1920), F32)],
        mib=60,
    )
    got = a2a(send, SP)
    state_sent, table = call(prefix_body, q, (got,), [((64, 8, 128), BF), ((16, 128), F32)])
    state = a2a(state_sent, SP).reshape(slots, 128)
    nbf, back = call(
        normed_body, q, (state, pack), [((n, heads * vd), BF), ((n, 896), F32)],
        hbm_out=(0, 1),
    )
    along = [nbf] + [lax.ppermute(nbf, "sp_1", [(i, (i + by) % 4) for i in range(4)]) for by in (3, 2, 1)]
    nball = along + [lax.ppermute(a, "sp_2", [(0, 1), (1, 0)]) for a in along]

    wrow = (quarter, hidden)
    gspec = {k: block_rows(k, wrow) for k in range(4)}
    dspec = {k: block_cols(k, (hidden, quarter)) for k in range(4)}
    near = (0, 1, 3)
    parts = call(
        early_body,
        q,
        (*[rows4[k] for k in near], *[grads4[k] for k in near], *[gate_w] * 3, *[up_w] * 3, *[down_w] * 3),
        [((slots, hidden), F32)] * 3,
        in_specs={6 + i: gspec[k] for i, k in enumerate(near)}
        | {9 + i: gspec[k] for i, k in enumerate(near)}
        | {12 + i: dspec[k] for i, k in enumerate(near)},
        mib=20,
    )
    half = slots // 2
    act, gp, up, far_lo, far_hi = call(
        hidden_grads_body,
        q,
        (rows4[2], grads4[2], down_w, gate_w, up_w, *parts),
        [((slots, hidden), BF)] * 3 + [((half, quarter), BF)] * 2,
        in_specs={2: dspec[2], 3: gspec[2], 4: gspec[2]},
        mib=20,
        hbm_out=range(5),
    )
    right_lo, right_hi, left_lo, left_hi, mine = call(
        expert_back_body,
        q,
        (gp, up, *[gate_w] * 3, *[up_w] * 3),
        [((half, quarter), BF)] * 4 + [((slots, quarter), BF)],
        in_specs={2 + i: gspec[k] for i, k in enumerate(near)} | {5 + i: gspec[k] for i, k in enumerate(near)},
        mib=20,
        hbm_in=(0, 1),
        hbm_out=range(5),
    )
    far_lo, far_hi = shift(far_lo, 1), shift(far_hi, 3)
    right_hi, left_lo = shift(right_hi, 1), shift(left_lo, 3)
    right_lo, left_hi = call(
        pass_on_body, q, (right_lo, far_lo, left_hi, far_hi), [((half, quarter), BF)] * 2,
        hbm_in=(0, 2),
    )
    right_lo, left_hi = shift(right_lo, 1), shift(left_hi, 3)
    gate_grad, up_grad, down_grad = call(
        weight_grads_body,
        q,
        (*rows4, *grads4, gp, up, act),
        [((width, hidden), BF), ((width, hidden), BF), ((hidden, width), BF)],
        out_specs={
            0: pl.BlockSpec(wrow, lambda i, q: (lax.rem(q[0] + i, 4), 0)),
            1: pl.BlockSpec(wrow, lambda i, q: (lax.rem(q[0] + i, 4), 0)),
            2: pl.BlockSpec((hidden, quarter), lambda i, q: (0, lax.rem(q[0] + i, 4))),
        },
        grid=4,
        mib=24,
    )
    (share,) = call(
        share_body, q, (mine, right_lo, right_hi, left_lo, left_hi), [((slots, quarter), BF)],
        hbm_in=(0,),
        hbm_out=(0,),
    )
    share = a2a(share.reshape(64, 8, quarter), SP).reshape(slots, quarter)
    (resid,) = call(combine_body, q, (share, qt, out_grad), [((n, quarter), BF)], in_specs={2: own}, hbm_in=(1, 2))
    resid4 = around(resid)

    pspec = {4 + k: block_rows(k, (quarter, out_proj.shape[1])) for k in range(4)}
    rg, inner = call(
        inner_grad_body,
        q,
        (*resid4, *[out_proj] * 4, back),
        [((n, heads * vd), F32), ((8, 320, 128), BF)],
        in_specs=pspec,
        hbm_in=(8,),
        hbm_out=(0, 1),
    )
    inner = a2a(inner, YC)
    qg, rest = call(local_grads_body, q, (rg, vv, pack, state), [((n, heads, kd), BF), ((n, 768), F32)])
    inside, later = call(
        plane_body, q, (inner, *nball, table), [((8, 64, 128), F32), ((8, 192, 128), BF)], hbm_in=range(1, 9)
    )
    later = a2a(later, ZAX)
    future, proj_grad = call(planes_body, q, (later, inside, table), [((8, 64, 128), BF), ((32, heads * vd), F32)])
    future = a2a(future, YC).reshape(slots, 128)
    kg, vg = call(final_body, q, (future, vv, pack, rest), [((n, heads, kd), BF), ((n, heads, vd), BF)])
    return (
        gate_grad[None],
        up_grad[None],
        down_grad[None],
        proj_grad,
        qg,
        kg,
        vg,
    )


def solution(mesh):
    split = Mesh(mesh.devices.reshape(8, 4, 2, mesh.shape["tp"]), (*SP, TP))
    placed = (
        P(SP, None),
        P(SP, None),
        P(SP, None),
        P(SP, None),
        P(SP, TP, None),
        P(SP, TP, None),
        P(SP, TP, None),
        P(SP, TP),
        P(None, TP),
        P(SP, None, TP),
        P(SP, None, TP),
        P(SP, TP, None),
    )

    return jax.shard_map(
        per_device,
        mesh=split,
        in_specs=placed,
        out_specs=(
            P(SP, None, TP),
            P(SP, None, TP),
            P(SP, TP, None),
            P(SP, TP),
            P(SP, TP, None),
            P(SP, TP, None),
            P(SP, TP, None),
        ),
        check_vma=False,
    )
```

```python
import jax
import jax.numpy as jnp
from jax import lax
from jax.experimental import pallas as pl
from jax.experimental.pallas import tpu as pltpu
from jax.sharding import Mesh
from jax.sharding import PartitionSpec as P


SP = ("sp_0", "sp_1", "sp_2")
YC = ("sp_1", "sp_2")
ZAX = "sp_0"
TP = "tp"


CLAMP_LIMIT = 7.0
GATE_SLOPE = 1.702
EPSILON = 1e-06
HI = lax.Precision.HIGHEST
F32 = jnp.float32
BF = jnp.bfloat16

NN = (((1,), (0,)), ((), ()))
NT = (((1,), (1,)), ((), ()))
TN = (((0,), (0,)), ((), ()))


def mm(a, b, dims=NN):
    return lax.dot_general(a, b, dims, preferred_element_type=F32)


def mmh(a, b, dims=NN):
    return lax.dot_general(a, b, dims, precision=HI, preferred_element_type=F32)


def mms(a, b, dims=NN):
    def parts(x):
        if x.dtype == BF:
            return [x]
        hi = x.astype(BF)
        return [hi, (x - hi.astype(F32)).astype(BF)]

    pa, pb = parts(a), parts(b)
    out = mm(pa[0], pb[0], dims)
    for x in pa[1:]:
        out = out + mm(x, pb[0], dims)
    for x in pb[1:]:
        out = out + mm(pa[0], x, dims)
    return out


def iota(shape, dim):
    return lax.broadcasted_iota(jnp.int32, shape, dim)


def whole(shape):
    return pl.BlockSpec(shape, lambda i, q: (0,) * len(shape))


def call(body, q, args, outs, in_specs=None, out_specs=None, grid=1, after=(), mib=16, hbm_in=(), hbm_out=()):
    in_specs = dict(in_specs or {})
    out_specs = out_specs or {}
    used = len(args)
    args = (*args, *after)
    args = tuple(pltpu.with_memory_space_constraint(a, pltpu.HBM) if i in hbm_in else a for i, a in enumerate(args))
    for i in range(used, len(args)):
        in_specs[i] = pl.BlockSpec(memory_space=pltpu.HBM)

    def kernel(q_ref, *refs):
        body(q_ref, *refs[:used], *refs[len(args) :])

    return pl.pallas_call(
        kernel,
        out_shape=[(pltpu.HBM if i in hbm_out else jax.ShapeDtypeStruct)(s, d) for i, (s, d) in enumerate(outs)],
        grid_spec=pltpu.PrefetchScalarGridSpec(
            num_scalar_prefetch=1,
            grid=(grid,),
            in_specs=[in_specs.get(i, whole(a.shape)) for i, a in enumerate(args)],
            out_specs=[out_specs.get(i, whole(s)) for i, (s, _) in enumerate(outs)],
        ),
        compiler_params=pltpu.CompilerParams(vmem_limit_bytes=mib << 20),
    )(q, *args)


def slots_of(routes):
    n = routes.shape[1]
    ti, tj = iota((n, n), 0), iota((n, n), 1)
    eye = ti == tj
    before = ti < tj
    r = routes[...].astype(F32)

    def col(c):
        return jnp.sum(jnp.where(eye, c, 0.0), axis=1, keepdims=True)

    e0r, e1r = r[0:1], r[1:2]
    e0, e1 = col(e0r), col(e1r)

    def earlier(er):
        same = (e0 == er).astype(F32) + (e1 == er).astype(F32)
        return jnp.sum(jnp.where(before, same, 0.0), axis=0, keepdims=True)

    cap = 8
    d0 = e0r * cap + earlier(e0r)
    d1 = e1r * cap + earlier(e1r) + (e0r == e1r).astype(F32)
    return d0, d1, col


def dispatch_body(q, routes, rw, stream, og, send):
    n = routes.shape[1]
    slots = send.shape[0] * 8
    d0, d1, _ = slots_of(routes)
    w = rw[...]
    di = iota((slots, n), 0).astype(F32)
    q0, q1 = di == d0, di == d1
    weight = jnp.where(q0, w[0:1], 0.0) + jnp.where(q1, w[1:2], 0.0)
    weight = jnp.sum(weight, axis=1, keepdims=True)
    pick = (jnp.where(q0, 1.0, 0.0) + jnp.where(q1, 1.0, 0.0)).astype(BF)
    rows = mm(pick, stream[...]).reshape(64, 8, -1)
    grads = (mm(pick, og[...]) * weight).reshape(64, 8, -1)
    send[...] = jnp.concatenate([rows, grads], axis=1).astype(BF)


def back_picks_body(q, routes, qt):
    n, slots = routes.shape[1], qt.shape[1]
    d0, d1, col = slots_of(routes)
    dl = iota((n, slots), 1).astype(F32)
    qt[0:n, :] = jnp.where(dl == col(d0), 1.0, 0.0).astype(BF)
    qt[n : 2 * n, :] = jnp.where(dl == col(d1), 1.0, 0.0).astype(BF)


def combine_body(q, ret, qt, og, resid):
    n = og.shape[0]
    back = mm(qt[...], ret[...])
    resid[...] = ((og[...].astype(F32) + back[0:n]) + back[n : 2 * n]).astype(BF)


def early_body(q, r0, r1, r3, x0, x1, x3, g0, g1, g3, u0, u1, u3, d0, d1, d3, gate, up, act_grad):
    a, b, c = r0[...], r1[...], r3[...]
    gate[...] = mm(a, g0[...]) + mm(b, g1[...]) + mm(c, g3[...])
    up[...] = mm(a, u0[...]) + mm(b, u1[...]) + mm(c, u3[...])
    act_grad[...] = mm(x0[...], d0[...], NT) + mm(x1[...], d1[...], NT) + mm(x3[...], d3[...], NT)


def hidden_grads_body(q, r2, x2, d2, g2, u2, gate_part, up_part, act_part, act, gp, up, far_lo, far_hi):
    x = r2[...]
    gate = gate_part[...] + mm(x, g2[...])
    upv = up_part[...] + mm(x, u2[...])
    act_grad = act_part[...] + mm(x2[...], d2[...], NT)
    gc = jnp.minimum(gate, CLAMP_LIMIT)
    uc = jnp.clip(upv, -CLAMP_LIMIT, CLAMP_LIMIT)
    sig = 1.0 / (1.0 + jnp.exp(-GATE_SLOPE * gc))
    gs = gc * sig
    act[...] = (gs * (uc + 1.0)).astype(BF)
    slope = sig + GATE_SLOPE * gs * (1.0 - sig)
    gpg = jnp.where(gate < CLAMP_LIMIT, act_grad * (uc + 1.0) * slope, 0.0).astype(BF)
    upg = jnp.where(jnp.abs(upv) < CLAMP_LIMIT, act_grad * gs, 0.0).astype(BF)
    gp[...] = gpg
    up[...] = upg
    half = far_lo.shape[0]
    part = (mm(gpg, g2[...], NT) + mm(upg, u2[...], NT)).astype(BF)
    far_lo[...] = part[:half]
    far_hi[...] = part[half:]


def expert_back_body(q, gp, up, g0, g1, g3, u0, u1, u3, right_lo, right_hi, left_lo, left_hi, mine):
    gpg, upg = gp[...], up[...]

    def back(g, u):
        return (mm(gpg, g[...], NT) + mm(upg, u[...], NT)).astype(BF)

    half = right_lo.shape[0]
    for lo, hi, part in ((right_lo, right_hi, back(g1, u1)), (left_lo, left_hi, back(g3, u3))):
        lo[...] = part[:half]
        hi[...] = part[half:]
    mine[...] = back(g0, u0)


def weight_grads_body(q, r0, r1, r2, r3, x0, x1, x2, x3, gp, up, act, gw, uw, dw):
    step = pl.program_id(0)
    for k, (r, x) in enumerate(zip((r0, r1, r2, r3), (x0, x1, x2, x3))):

        @pl.when(step == k)
        def _(r=r, x=x):
            rt = r[...]
            gw[...] = mm(rt, gp[...], TN).astype(BF)
            uw[...] = mm(rt, up[...], TN).astype(BF)
            dw[...] = mm(act[...], x[...], TN).astype(BF)


def pass_on_body(q, right_lo, far_lo, left_hi, far_hi, right, left):
    right[...] = (right_lo[...].astype(F32) + far_lo[...].astype(F32)).astype(BF)
    left[...] = (left_hi[...].astype(F32) + far_hi[...].astype(F32)).astype(BF)


def share_body(q, mine, a_lo, a_hi, b_lo, b_hi, out):
    half = a_lo.shape[0]
    m = mine[...].astype(F32)
    out[:half, :] = (m[:half] + (a_lo[...].astype(F32) + b_lo[...].astype(F32))).astype(BF)
    out[half:, :] = (m[half:] + (a_hi[...].astype(F32) + b_hi[...].astype(F32))).astype(BF)


def weight_grads_body(q, r0, r1, r2, r3, x0, x1, x2, x3, gp, up, act, gw, uw, dw):
    step = pl.program_id(0)
    for k, (r, x) in enumerate(zip((r0, r1, r2, r3), (x0, x1, x2, x3))):

        @pl.when(step == k)
        def _(r=r, x=x):
            rt = r[...]
            gw[...] = mm(rt, gp[...], TN).astype(BF)
            uw[...] = mm(rt, up[...], TN).astype(BF)
            dw[...] = mm(act[...], x[...], TN).astype(BF)


def turned(x, c, s):
    even = (iota(x.shape, 1) % 2) == 0
    n = x.shape[1]
    other = jnp.where(even, -pltpu.roll(x, n - 1, 1), pltpu.roll(x, 1, 1))
    return x * c + other * s


QR, KR, WTS, MASK, SCAL, COS, SIN, INTRA = 0, 256, 512, 768, 1024, 1152, 1280, 1408


def prepare_body(q, qv, kv, vv, ld, cb, sb, cr, sr, send, pack):
    heads, n, kd = qv.shape
    vd = vv.shape[2]
    ti, tj = iota((n, n), 0), iota((n, n), 1)
    eye, causal = ti == tj, ti >= tj
    c = cb[...] * cr[...] - sb[...] * sr[...]
    s = sb[...] * cr[...] + cb[...] * sr[...]
    pack[:, COS : COS + kd] = c
    pack[:, SIN : SIN + kd] = s
    pieces = []
    logs = jnp.zeros((1, 8, 128), F32)
    sub = iota((1, 8, 128), 1)
    scal = jnp.zeros((n, 128), F32)
    lane = iota((n, 128), 1)
    for h in range(heads):
        col = jnp.sum(jnp.where(eye, ld[h : h + 1, :], 0.0), axis=1, keepdims=True)
        rt_r = jnp.sum(jnp.where(ti <= tj, col, 0.0), axis=0, keepdims=True)
        rt_c = jnp.sum(jnp.where(eye, rt_r, 0.0), axis=1, keepdims=True)
        total = rt_r[:, n - 1 : n]
        mask = jnp.where(causal, jnp.exp(jnp.where(causal, rt_c - rt_r, 0.0)), 0.0)
        grow = jnp.exp(rt_c)
        left = jnp.exp(total - rt_c)
        qh = turned(qv[h].astype(F32), c, s)
        kh = turned(kv[h].astype(F32), c, s) * (kd**-0.5)
        vh = vv[h]
        inner = mms((kh * left).T, vh)
        for u in range(vd // 128):
            pieces.append(inner[:, u * 128 : (u + 1) * 128])
        hi = total.astype(BF).astype(F32)
        mid = (total - hi).astype(BF).astype(F32)
        for k, part in enumerate((hi, mid, total - hi - mid)):
            logs = jnp.where(sub == 3 * h + k, part[None], logs)
        w = mms(qh, kh, NT) * mask
        pack[:, INTRA + h * vd : INTRA + (h + 1) * vd] = mms(w, vh)
        at = h * 128
        pack[:, QR + at : QR + at + 128] = qh
        pack[:, KR + at : KR + at + 128] = kh
        pack[:, WTS + at : WTS + at + 128] = w
        pack[:, MASK + at : MASK + at + 128] = mask
        scal = jnp.where(lane == h, grow, jnp.where(lane == 2 + h, left, scal))
    pack[:, SCAL : SCAL + 128] = scal
    state = jnp.concatenate(pieces, axis=0).reshape(-1, 8, 128)
    send[...] = jnp.concatenate([state, jnp.broadcast_to(logs, state.shape)], axis=1).astype(BF)


def prefix_body(q, x, out, table):
    n = x.shape[0]
    z, j = q[1], q[2]
    xf = x[...].astype(F32)
    logs = [xf[:, 8 + 3 * h, :] + xf[:, 9 + 3 * h, :] + xf[:, 10 + 3 * h, :] for h in range(2)]
    mine = jnp.where(z >= 4, logs[1], logs[0])[:, 0:1]
    ti, tj = iota((n, n), 0), iota((n, n), 1)
    after = jnp.where(ti > tj, mine, 0.0)
    seg = mmh(jnp.where(tj < ti, 1.0, 0.0), after)
    w = jnp.where(tj < ti, jnp.exp(seg), 0.0)
    acc = mmh(w, jnp.concatenate([xf[:, k, :] for k in range(8)], axis=1))
    out[...] = jnp.stack([acc[:, k * 128 : (k + 1) * 128] for k in range(8)], axis=1).astype(BF)
    other = jnp.where(j >= 4, logs[1], logs[0])[:, 0:1]
    row = jnp.sum(jnp.where(ti == tj, other, 0.0), axis=0, keepdims=True)
    i, m = iota((16, n), 0), iota((16, n), 1)
    low = jnp.where(i == 8, 8 * z - 1, 8 * z + i)
    a = jnp.where((m > low) & (i < 9), row, 0.0)
    m2, c2 = iota((n, 128), 0), iota((n, 128), 1)
    high = jnp.where(c2 < 16, 8 * z + c2, 8 * (c2 - 16))
    b = jnp.where(m2 < high, 1.0, 0.0)
    decay = jnp.exp(mmh(a, b))
    i, c = iota((16, 128), 0), iota((16, 128), 1)
    used = ((c < 8) & ((i == 8) | (c > i))) | ((c == 8) & (i < 8)) | ((i == 7) & (c >= 16) & (c < 24) & (c - 16 > z))
    table[...] = jnp.where(used, decay, 0.0)


def joined(state, h, vd):
    per = vd // 128
    base = h * per * 128
    return jnp.concatenate([state[base + u * 128 : base + (u + 1) * 128, :] for u in range(per)], axis=1)


INV, QDT = 512, 640


def normed_body(q, state, pack, nbf, back):
    n = pack.shape[0]
    heads, vd = 2, 256
    st = state[...]
    lane = iota((n, 128), 1)
    invs = jnp.zeros((n, 128), F32)
    for h in range(heads):
        sl = slice(h * vd, (h + 1) * vd)
        qh = pack[:, QR + h * 128 : QR + (h + 1) * 128]
        grow = pack[:, SCAL + h : SCAL + h + 1]
        ret = pack[:, INTRA + h * vd : INTRA + (h + 1) * vd] + grow * mms(qh, joined(st, h, vd))
        iv = lax.rsqrt(jnp.mean(ret * ret, axis=1, keepdims=True) + EPSILON)
        nm = ret * iv
        back[:, sl] = nm
        nbf[:, sl] = nm.astype(BF)
        invs = jnp.where(lane == h, iv, invs)
        back[:, QDT + h * 128 : QDT + (h + 1) * 128] = (qh * grow).T
    back[:, INV : INV + 128] = invs


def inner_grad_body(q, r0, r1, r2, r3, p0, p1, p2, p3, back, rg, send):
    heads, vd = 2, 256
    ng = mm(r0[...], p0[...])
    for r, p in zip((r1, r2, r3), (p1, p2, p3)):
        ng = ng + mm(r[...], p[...])
    for h in range(heads):
        sl = slice(h * vd, (h + 1) * vd)
        nm, g = back[:, sl], ng[:, sl]
        m = jnp.mean(g * nm, axis=1, keepdims=True)
        grad = back[:, INV + h : INV + h + 1] * (g - nm * m)
        rg[:, sl] = grad
        inner = mms(back[:, QDT + h * 128 : QDT + (h + 1) * 128], grad)
        for u in range(vd // 128):
            for e in range(2):
                part = inner[e * 64 : (e + 1) * 64, u * 128 : (u + 1) * 128]
                send[h * 4 + u * 2 + e, 0:64, :] = part.astype(BF)
    for k, r in enumerate((r0, r1, r2, r3)):
        block = lax.rem(q[0] + k, 4)
        t = r[...].astype(F32).T.astype(BF)
        for lo in range(2):
            at = pl.multiple_of(64 + (block * 2 + lo) * 32, 32)
            for j in range(8):
                src = lo * 256 + j * 32
                send[j, pl.ds(at, 32), :] = t[src : src + 32, :]


def local_grads_body(q, rg, vv, pack, state, qg, rest):
    heads, vd = 2, 256
    parts = []
    st = state[...]
    c, s = pack[:, COS : COS + 128], pack[:, SIN : SIN + 128]
    for h in range(heads):
        at = h * 128
        grad = rg[:, h * vd : (h + 1) * vd]
        score = mms(grad, vv[h], NT) * pack[:, MASK + at : MASK + at + 128]
        grow = pack[:, SCAL + h : SCAL + h + 1]
        qp = mms(score, pack[:, KR + at : KR + at + 128]) + grow * mms(grad, joined(st, h, vd), NT)
        parts.append(turned(qp, c, -s))
        rest[:, at : at + 128] = mms(score.T, pack[:, QR + at : QR + at + 128])
        rest[:, 256 + h * vd : 256 + (h + 1) * vd] = mms(pack[:, WTS + at : WTS + at + 128].T, grad)
    qg[...] = jnp.stack(parts, axis=1).astype(BF)


def plane_body(q, x, n0, n1, n2, n3, m0, m1, m2, m3, table, inside, send):
    blocks = x.shape[0]
    parts = [x[k, 0:64, :].astype(F32) for k in range(blocks)]
    for k in range(blocks):
        acc = jnp.zeros((64, 128), F32)
        for m in range(k + 1, blocks):
            acc = acc + table[k : k + 1, m : m + 1] * parts[m]
        inside[k] = acc
    total = jnp.zeros((64, 128), F32)
    for m in range(blocks):
        total = total + table[8:9, m : m + 1] * parts[m]
    total = total.astype(BF)
    proj = 0.0
    y, core = q[2] // 2, q[2] % 2
    for k, nb in enumerate((n0, n1, n2, n3)):
        proj = proj + mm(x[lax.rem(y + k, 4) * 2 + core, 64:320, :], nb[...])
    for k, nb in enumerate((m0, m1, m2, m3)):
        proj = proj + mm(x[lax.rem(y + k, 4) * 2 + 1 - core, 64:320, :], nb[...])
    for k in range(blocks):
        send[k, 0:64, :] = total
        for u in range(4):
            send[k, 64 + u * 32 : 96 + u * 32, :] = proj[k * 32 : (k + 1) * 32, u * 128 : (u + 1) * 128].astype(BF)


def planes_body(q, y, inside, table, out, proj):
    blocks = y.shape[0]
    later = jnp.zeros((64, 128), F32)
    for k in range(blocks):
        later = later + table[7:8, 16 + k : 17 + k] * y[k, 0:64, :].astype(F32)
    for k in range(blocks):
        out[k] = (inside[k] + table[k : k + 1, 8:9] * later).astype(BF)
    for u in range(4):
        acc = y[0, 64 + u * 32 : 96 + u * 32, :].astype(F32)
        for k in range(1, blocks):
            acc = acc + y[k, 64 + u * 32 : 96 + u * 32, :].astype(F32)
        proj[:, u * 128 : (u + 1) * 128] = acc


def final_body(q, state, vv, pack, rest, kg, vg):
    heads, vd, kd = 2, 256, 128
    keys, values = [], []
    st = state[...]
    c, s = pack[:, COS : COS + 128], pack[:, SIN : SIN + 128]
    for h in range(heads):
        at = h * 128
        fut = joined(st, h, vd)
        left = pack[:, SCAL + 2 + h : SCAL + 3 + h]
        kt = rest[:, at : at + 128] + left * mms(vv[h], fut, NT)
        keys.append(turned(kt, c, -s) * (kd**-0.5))
        vt = rest[:, 256 + h * vd : 256 + (h + 1) * vd]
        values.append(vt + left * mms(pack[:, KR + at : KR + at + 128], fut))
    kg[...] = jnp.stack(keys, axis=1).astype(BF)
    vg[...] = jnp.stack(values, axis=1).astype(BF)


def a2a(x, axes):
    return lax.all_to_all(x, axes, split_axis=0, concat_axis=0, tiled=True)


def shift(x, by):
    return lax.ppermute(x, TP, [(i, (i + by) % 4) for i in range(4)])


def around(x):
    far = shift(x, 2)
    return x, shift(x, 3), far, shift(x, 1)


def block_rows(k, shape):
    return pl.BlockSpec(shape, lambda i, q, k=k: (lax.rem(q[0] + k, 4), 0))


def block_cols(k, shape):
    return pl.BlockSpec(shape, lambda i, q, k=k: (0, lax.rem(q[0] + k, 4)))


def per_device(
    stream,
    out_grad,
    routes,
    route_weight,
    queries,
    key_vectors,
    value_vectors,
    log_decay,
    out_proj,
    gate_weight,
    up_weight,
    down_weight,
):
    n, width = stream.shape
    quarter = width // 4
    slots = 512
    hidden = gate_weight.shape[2]
    heads, kd = queries.shape[1:]
    vd = value_vectors.shape[2]
    sp = lax.axis_index(SP)
    q = jnp.stack([lax.axis_index(TP), sp // 8, sp % 8, sp]).astype(jnp.int32)
    gate_w, up_w, down_w = gate_weight[0], up_weight[0], down_weight[0]

    own = pl.BlockSpec((n, quarter), lambda i, q: (0, q[0]))
    (sent,) = call(
        dispatch_body,
        q,
        (routes.T, route_weight.T, stream, out_grad),
        [((64, 16, quarter), BF)],
        in_specs={2: own, 3: own},
        mib=60,
    )
    came = a2a(sent, SP)
    rows = came[:, :8].reshape(slots, quarter)
    grads = came[:, 8:].reshape(slots, quarter)
    rows_prev, rows_next = shift(rows, 1), shift(rows, 3)
    grads_prev, grads_next = shift(grads, 1), shift(grads, 3)
    rows_far, grads_far = shift(rows_prev, 1), shift(grads_next, 3)
    rows4 = (rows, rows_next, rows_far, rows_prev)
    grads4 = (grads, grads_next, grads_far, grads_prev)

    freq = 1.0 / 10000.0 ** jnp.linspace(0.0, 1.0, kd // 2, dtype=F32)
    freq = jnp.repeat(freq, 2)[None, :]
    base = (sp * n).astype(F32) * freq
    angles = jnp.arange(n, dtype=F32)[:, None] * freq
    qv = queries.transpose(1, 0, 2)
    kv = key_vectors.transpose(1, 0, 2)
    vv = value_vectors.transpose(1, 0, 2)
    (qt,) = call(back_picks_body, q, (routes.T,), [((2 * n, slots), BF)], hbm_out=(0,))
    send, pack = call(
        prepare_body,
        q,
        (qv, kv, vv, log_decay.T, jnp.cos(base), jnp.sin(base), jnp.cos(angles), jnp.sin(angles)),
        [((64, 16, 128), BF), ((n, 1920), F32)],
        mib=60,
    )
    got = a2a(send, SP)
    state_sent, table = call(prefix_body, q, (got,), [((64, 8, 128), BF), ((16, 128), F32)])
    state = a2a(state_sent, SP).reshape(slots, 128)
    nbf, back = call(
        normed_body, q, (state, pack), [((n, heads * vd), BF), ((n, 896), F32)],
        hbm_out=(0, 1),
    )
    along = [nbf] + [lax.ppermute(nbf, "sp_1", [(i, (i + by) % 4) for i in range(4)]) for by in (3, 2, 1)]
    nball = along + [lax.ppermute(a, "sp_2", [(0, 1), (1, 0)]) for a in along]

    wrow = (quarter, hidden)
    gspec = {k: block_rows(k, wrow) for k in range(4)}
    dspec = {k: block_cols(k, (hidden, quarter)) for k in range(4)}
    near = (0, 1, 3)
    parts = call(
        early_body,
        q,
        (*[rows4[k] for k in near], *[grads4[k] for k in near], *[gate_w] * 3, *[up_w] * 3, *[down_w] * 3),
        [((slots, hidden), F32)] * 3,
        in_specs={6 + i: gspec[k] for i, k in enumerate(near)}
        | {9 + i: gspec[k] for i, k in enumerate(near)}
        | {12 + i: dspec[k] for i, k in enumerate(near)},
        mib=20,
    )
    half = slots // 2
    act, gp, up, far_lo, far_hi = call(
        hidden_grads_body,
        q,
        (rows4[2], grads4[2], down_w, gate_w, up_w, *parts),
        [((slots, hidden), BF)] * 3 + [((half, quarter), BF)] * 2,
        in_specs={2: dspec[2], 3: gspec[2], 4: gspec[2]},
        mib=20,
        hbm_out=range(5),
    )
    right_lo, right_hi, left_lo, left_hi, mine = call(
        expert_back_body,
        q,
        (gp, up, *[gate_w] * 3, *[up_w] * 3),
        [((half, quarter), BF)] * 4 + [((slots, quarter), BF)],
        in_specs={2 + i: gspec[k] for i, k in enumerate(near)} | {5 + i: gspec[k] for i, k in enumerate(near)},
        mib=20,
        hbm_in=(0, 1),
        hbm_out=range(5),
    )
    far_lo, far_hi = shift(far_lo, 1), shift(far_hi, 3)
    right_hi, left_lo = shift(right_hi, 1), shift(left_lo, 3)
    right_lo, left_hi = call(
        pass_on_body, q, (right_lo, far_lo, left_hi, far_hi), [((half, quarter), BF)] * 2,
        hbm_in=(0, 2),
    )
    right_lo, left_hi = shift(right_lo, 1), shift(left_hi, 3)
    gate_grad, up_grad, down_grad = call(
        weight_grads_body,
        q,
        (*rows4, *grads4, gp, up, act),
        [((width, hidden), BF), ((width, hidden), BF), ((hidden, width), BF)],
        out_specs={
            0: pl.BlockSpec(wrow, lambda i, q: (lax.rem(q[0] + i, 4), 0)),
            1: pl.BlockSpec(wrow, lambda i, q: (lax.rem(q[0] + i, 4), 0)),
            2: pl.BlockSpec((hidden, quarter), lambda i, q: (0, lax.rem(q[0] + i, 4))),
        },
        grid=4,
        mib=24,
    )
    (share,) = call(
        share_body, q, (mine, right_lo, right_hi, left_lo, left_hi), [((slots, quarter), BF)],
        hbm_in=(0,),
        hbm_out=(0,),
    )
    share = a2a(share.reshape(64, 8, quarter), SP).reshape(slots, quarter)
    (resid,) = call(combine_body, q, (share, qt, out_grad), [((n, quarter), BF)], in_specs={2: own}, hbm_in=(1, 2))
    resid4 = around(resid)

    pspec = {4 + k: block_rows(k, (quarter, out_proj.shape[1])) for k in range(4)}
    rg, inner = call(
        inner_grad_body,
        q,
        (*resid4, *[out_proj] * 4, back),
        [((n, heads * vd), F32), ((8, 320, 128), BF)],
        in_specs=pspec,
        hbm_in=(8,),
        hbm_out=(0, 1),
    )
    inner = a2a(inner, YC)
    qg, rest = call(local_grads_body, q, (rg, vv, pack, state), [((n, heads, kd), BF), ((n, 768), F32)])
    inside, later = call(
        plane_body, q, (inner, *nball, table), [((8, 64, 128), F32), ((8, 192, 128), BF)], hbm_in=range(1, 9)
    )
    later = a2a(later, ZAX)
    future, proj_grad = call(planes_body, q, (later, inside, table), [((8, 64, 128), BF), ((32, heads * vd), F32)])
    future = a2a(future, YC).reshape(slots, 128)
    kg, vg = call(final_body, q, (future, vv, pack, rest), [((n, heads, kd), BF), ((n, heads, vd), BF)])
    return (
        gate_grad[None],
        up_grad[None],
        down_grad[None],
        proj_grad,
        qg,
        kg,
        vg,
    )


def solution(mesh):
    split = Mesh(mesh.devices.reshape(8, 4, 2, mesh.shape["tp"]), (*SP, TP))
    placed = (
        P(SP, None),
        P(SP, None),
        P(SP, None),
        P(SP, None),
        P(SP, TP, None),
        P(SP, TP, None),
        P(SP, TP, None),
        P(SP, TP),
        P(None, TP),
        P(SP, None, TP),
        P(SP, None, TP),
        P(SP, TP, None),
    )

    return jax.shard_map(
        per_device,
        mesh=split,
        in_specs=placed,
        out_specs=(
            P(SP, None, TP),
            P(SP, None, TP),
            P(SP, TP, None),
            P(SP, TP),
            P(SP, TP, None),
            P(SP, TP, None),
            P(SP, TP, None),
        ),
        check_vma=False,
    )
```
